512 devices in a mesh: ep: 32 (over z, x), tp: 16 (over y, core).
Axes of the slice: x: 4, y: 8, z: 8, core: 2. Of those that a mesh axis runs over, the one named last changes fastest.
Arguments:
- mixer_rows: bfloat16 [4096, 2048], P('ep'), may hold values from -40 to 40
- mixer_gain: float32 [2048], replicated, may hold values from 0.1 to 1.9
- inner_weight: bfloat16 [2048, 1024], P(None, 'tp'), may hold values from -0.125 to 0.125
- gate_in_weight: bfloat16 [2048, 1024], P(None, 'tp'), may hold values from -0.125 to 0.125
- gate_out_weight: bfloat16 [2048, 1024], P(None, 'tp'), may hold values from -0.125 to 0.125
- conv_taps: float32 [3, 1024], P(None, 'tp'), may hold values from -3.5 to 3.5
- mixer_out_weight: bfloat16 [1024, 2048], P('tp'), may hold values from -0.1875 to 0.1875
- routed_rows: bfloat16 [8192, 2048], P('ep'), may hold values from -40 to 40
- routed_gain: float32 [2048], replicated, may hold values from 0.1 to 1.9
- route_ids: int32 [8192, 2], P('ep'), may hold values from 0 to 31, all different within a row; in each aligned block of 256 rows (0 to 255, 256 to 511, ...) at most 32 rows name the same one
- route_weights: float32 [8192, 2], P('ep'), may hold values from 0.25 to 1
- expert_gate: bfloat16 [32, 2048, 2048], P('ep', None, 'tp'), may hold values from -0.125 to 0.125
- expert_up: bfloat16 [32, 2048, 2048], P('ep', None, 'tp'), may hold values from -0.125 to 0.125
- expert_down: bfloat16 [32, 2048, 2048], P('ep', 'tp'), may hold values from -0.125 to 0.125
Outputs:
- mixer_output: bfloat16 [4096, 2048], P('ep')
- routed_output: bfloat16 [8192, 2048], P('ep')
The draws below stay inside these ranges and needn't reach their ends.
Inputs may be any that keep to these rules, and one draw needn't show every extreme that they name: `route_ids`: within each aligned block of 256 tokens, no expert is named by more than 32 choices, a bound that some block reaches; a token's 2 experts differ.
All inputs are finite; a program needn't handle non-finite values.
Results may differ from the reference program's by a relative error of at most 0.019.
Values may be sent and summed in bfloat16 or wider, within the bound.
A program may use at most 64 MiB of HBM per device.

```python
import math
import jax
import jax.numpy as jnp
import numpy as np
from jax import lax

D = 2048
CONV = 1024
TAPS = 3
FF = 2048
TOPK = 2
EXPERTS = 32
TOK2 = 256
TOKENS1 = 4096
TOKENS2 = 8192
CAP = 32
N_TP = 16


def scaled_rows(key, row_total, model_width):
    keys = jax.random.split(key, 3)
    row_scale = jnp.exp(jax.random.uniform(keys[0], (row_total, 1), jnp.float32) * math.log(10.0))
    col_scale = jnp.exp(jax.random.uniform(keys[1], (1, model_width), jnp.float32) * math.log(10.0))
    base = jnp.clip(jax.random.normal(keys[2], (row_total, model_width), jnp.float32), -4.0, 4.0)
    return (base * row_scale * col_scale * 0.1).astype(jnp.bfloat16)


def draw_mixer_rows(key, part):
    return scaled_rows(jax.random.fold_in(key, 11), TOKENS1, D)


def draw_routed_rows(key, part):
    return scaled_rows(jax.random.fold_in(key, 23), TOKENS2, D)


def steps_of(stream_key, shape, pieces, least, top_value):
    loudness, own = 1.0, jax.random.fold_in(stream_key, 6)
    for dim, blocks in pieces:
        steps = jnp.exp(jax.random.uniform(jax.random.fold_in(own, dim), (blocks,), jnp.float32, least / len(pieces), top_value / len(pieces)))
        loudness = loudness * jnp.repeat(steps, shape[dim] // blocks).reshape([-1 if axis == dim else 1 for axis in range(len(shape))])
    return loudness


def assign_block(stream_key, own, number, rows, count, top, most, lean):
    order = jax.random.permutation(stream_key, count)
    crowded, usual = load_shares(count, rows * top, most, lean, True), load_shares(count, rows * top, most, lean, False)
    places = jnp.arange(count)

    def named(sizes, turn):
        used = int((sizes > 0).sum())
        fixed = max(1, used // 4)
        passed = fixed + (places - fixed + turn * (used - fixed)) % max(1, count - fixed)
        return jnp.zeros((count,), jnp.int32).at[order[jnp.where(places < fixed, places, passed)]].set(jnp.asarray(sizes, jnp.int32))

    sizes = jnp.where(number % 4 == 0, named(crowded, number // 4), named(usual, number - number // 4 - 1))
    mixed = jax.random.permutation(jax.random.fold_in(own, 3), count)
    donor, taker = mixed[0:count // 2 * 2:2], mixed[1:count // 2 * 2:2]
    room = jnp.minimum(sizes[donor] - 1, most - sizes[taker]) // 2
    room = jnp.where((donor == order[0]) | (taker == order[0]) | (sizes[taker] == 0), 0, jnp.maximum(room, 0))
    passed = jax.random.randint(jax.random.fold_in(own, 4), (count // 2,), 0, 1 << 20) % (room + 1)
    sizes = sizes.at[donor].add(-passed).at[taker].add(passed)
    members = jnp.searchsorted(jnp.cumsum(sizes), jnp.arange(rows * top), side="right").astype(jnp.int32)
    listing = members.reshape(top, rows).T
    listing = listing[jax.random.permutation(jax.random.fold_in(own, 1), rows)]
    turn = jax.random.randint(jax.random.fold_in(own, 2), (rows, 1), 0, top)
    return jnp.take_along_axis(listing, (jnp.arange(top)[None, :] + turn) % top, axis=1)


def load_shares(number_of, total, limit, skew, full):
    loads = [(1 << 20) // math.isqrt(grade ** skew) + 1 for grade in range(1, number_of + 1)]
    largest = limit if full else min(limit, max(-(-total // number_of), total * loads[0] // sum(loads)))
    least = 1 if total - largest >= number_of - 1 else 0
    given, surplus = [largest] + [least] * (number_of - 1), total - largest - least * (number_of - 1)
    while surplus > 0:
        movable = [i for i in range(1, number_of) if given[i] < largest] or [i for i in range(1, number_of) if given[i] < limit]
        mass, left = sum([loads[i] for i in movable]), surplus
        for i in movable:
            extra = min(limit - given[i], max(1, left * loads[i] // mass), surplus)
            given[i] = given[i] + extra
            surplus = surplus - extra
    return np.array(given)


def noise(key, dims, scale, bound, cuts=(), kind=jnp.bfloat16):
    loudness = steps_of(key, dims, cuts, -0.22, 0.18) if cuts else 1.0
    entries = jax.random.normal(key, dims, jnp.float32) * scale * loudness
    return jnp.minimum(jnp.maximum(entries, -bound), bound).astype(kind)


def setup_inputs(seed: int = 0) -> dict:
    arg_keys = jax.random.split(jax.random.key(seed), 15)
    mixer_rows = draw_mixer_rows(jax.random.fold_in(arg_keys[14], 71), 0)
    mixer_gain = jnp.clip(1.0 + 0.18 * jax.random.normal(arg_keys[1], (D,), jnp.float32), 0.1, 1.9)
    inner_weight = noise(arg_keys[2], (D, CONV), D ** -0.5, 0.125, ((1, 16),))
    gate_in_weight = noise(arg_keys[3], (D, CONV), D ** -0.5, 0.125, ((1, 16),))
    gate_out_weight = noise(arg_keys[4], (D, CONV), D ** -0.5, 0.125, ((1, 16),))
    conv_taps = noise(arg_keys[5], (TAPS, CONV), TAPS ** -0.5, 3.5, ((1, 16),), jnp.float32)
    mixer_out_weight = noise(arg_keys[6], (CONV, D), CONV ** -0.5, 0.1875, ((0, 16),))
    routed_rows = draw_routed_rows(jax.random.fold_in(arg_keys[14], 71), 0)
    routed_gain = jnp.clip(1.0 + 0.18 * jax.random.normal(arg_keys[8], (D,), jnp.float32), 0.1, 1.9)
    route_ids_keys = jax.random.split(jax.random.fold_in(arg_keys[9], 1), TOKENS2 // TOK2)
    route_ids_turns = jax.random.permutation(jax.random.fold_in(arg_keys[9], 3), TOKENS2 // TOK2)
    route_ids = jax.vmap(lambda own, number: assign_block(jax.random.fold_in(arg_keys[9], 2), own, number, TOK2, EXPERTS, TOPK, CAP, 2))(route_ids_keys, route_ids_turns).reshape((TOKENS2, TOPK))
    route_weights = jnp.clip(0.25 + 0.75 * jax.random.uniform(arg_keys[10], (TOKENS2, TOPK), jnp.float32) ** steps_of(arg_keys[10], (TOKENS2, TOPK), ((0, 32),), -0.2, 0.2), 0.25, 1.0)
    expert_gate = noise(arg_keys[11], (EXPERTS, D, FF), D ** -0.5, 0.125, ((0, 32), (2, 16)))
    expert_up = noise(arg_keys[12], (EXPERTS, D, FF), D ** -0.5, 0.125, ((0, 32), (2, 16)))
    expert_down = noise(arg_keys[13], (EXPERTS, FF, D), FF ** -0.5, 0.125, ((0, 32), (1, 16)))
    return dict(mixer_rows=mixer_rows, mixer_gain=mixer_gain, inner_weight=inner_weight, gate_in_weight=gate_in_weight, gate_out_weight=gate_out_weight, conv_taps=conv_taps, mixer_out_weight=mixer_out_weight, routed_rows=routed_rows, routed_gain=routed_gain, route_ids=route_ids, route_weights=route_weights, expert_gate=expert_gate, expert_up=expert_up, expert_down=expert_down)


def rms_scale(row_block, gain_row):
    values = row_block.astype(jnp.float32)
    scaled = values * lax.rsqrt(lax.optimization_barrier(jnp.mean(values * values, axis=-1, keepdims=True)) + 1e-06)
    return (scaled * gain_row).astype(jnp.bfloat16)

def rounded_again(partial_value):
    return lax.optimization_barrier(partial_value.astype(jnp.bfloat16)).astype(jnp.float32)

def reference(mixer_rows, mixer_gain, inner_weight, gate_in_weight, gate_out_weight, conv_taps, mixer_out_weight, routed_rows, routed_gain, route_ids, route_weights, expert_gate, expert_up, expert_down):
    normed = rms_scale(mixer_rows, mixer_gain)
    inner_proj = jnp.dot(normed, inner_weight, preferred_element_type=jnp.float32)
    gate_in = jnp.dot(normed, gate_in_weight, preferred_element_type=jnp.float32)
    conv_input = (gate_in * inner_proj).astype(jnp.bfloat16)
    gate_out = jnp.dot(normed, gate_out_weight, preferred_element_type=jnp.float32)
    padded = jnp.concatenate([jnp.zeros((TAPS - 1, CONV), jnp.bfloat16), conv_input], axis=0).astype(jnp.float32)
    conv_out = jnp.zeros((TOKENS1, CONV), jnp.float32)
    for tap_index in range(TAPS):
        conv_out = conv_out + conv_taps[tap_index] * padded[tap_index:tap_index + TOKENS1]
    gated_conv = (gate_out * conv_out).astype(jnp.bfloat16)
    group_width = CONV // N_TP
    running = jnp.zeros((TOKENS1, D), jnp.float32)
    for piece_index in range(N_TP):
        lower_edge = piece_index * group_width
        partial_value = jnp.dot(gated_conv[:, lower_edge:lower_edge + group_width], mixer_out_weight[lower_edge:lower_edge + group_width], preferred_element_type=jnp.float32)
        running = running + rounded_again(partial_value)
    mixer_output = running.astype(jnp.bfloat16)
    routed_normed = rms_scale(routed_rows, routed_gain)
    blocks = TOKENS2 // TOK2
    flat_ids = route_ids.reshape(blocks, TOK2 * TOPK).astype(jnp.int32)
    onehot = (flat_ids[:, :, None] == jnp.arange(EXPERTS, dtype=jnp.int32)[None, None, :]).astype(jnp.int32)
    earlier = (jnp.cumsum(onehot, axis=1) - onehot).astype(jnp.int32)
    slot_rank = lax.optimization_barrier(jnp.sum(earlier * onehot, axis=2)).astype(jnp.int32)
    block_grid = jnp.broadcast_to(jnp.arange(blocks, dtype=jnp.int32)[:, None], flat_ids.shape)
    token_index = (block_grid * TOK2 + jnp.arange(TOK2 * TOPK, dtype=jnp.int32)[None, :] // TOPK).astype(jnp.int32)
    token_table = jnp.full((EXPERTS, blocks, CAP), TOKENS2, jnp.int32).at[flat_ids, block_grid, slot_rank].set(token_index)
    padded_rows = jnp.concatenate([routed_normed, jnp.zeros((1, D), jnp.bfloat16)], axis=0)
    hidden_width = FF // N_TP

    def one_expert(operands):
        table_rows, gate_w, up_w, down_w = operands
        slot_rows = padded_rows[table_rows.reshape(-1)]
        gate_act = jnp.dot(slot_rows, gate_w, preferred_element_type=jnp.float32)
        up_act = jnp.dot(slot_rows, up_w, preferred_element_type=jnp.float32)
        hidden = (jax.nn.silu(gate_act) * up_act).astype(jnp.bfloat16)
        summed = jnp.zeros((slot_rows.shape[0], D), jnp.float32)
        for piece_index in range(N_TP):
            lower_edge = piece_index * hidden_width
            partial_value = jnp.dot(hidden[:, lower_edge:lower_edge + hidden_width], down_w[lower_edge:lower_edge + hidden_width], preferred_element_type=jnp.float32)
            summed = summed + rounded_again(partial_value)
        return summed.astype(jnp.bfloat16)
    results = lax.map(one_expert, (token_table, expert_gate, expert_up, expert_down))
    results = results.reshape(EXPERTS, blocks, CAP, D)
    picked = results[flat_ids, block_grid, slot_rank].reshape(TOKENS2, TOPK, D).astype(jnp.float32)
    picked = picked * route_weights[:, :, None]
    owner_piece = (slot_rank // (CAP // N_TP)).reshape(TOKENS2, TOPK)
    running_two = jnp.zeros((TOKENS2, D), jnp.float32)
    for piece_index in range(N_TP):
        partial_value = lax.optimization_barrier(jnp.sum(jnp.where((owner_piece == piece_index)[:, :, None], picked, jnp.float32(0.0)), axis=1))
        running_two = running_two + rounded_again(partial_value)
    routed_output = running_two.astype(jnp.bfloat16)
    return (mixer_output, routed_output)
```

```python
import functools

import jax
import jax.numpy as jnp
from jax import lax
from jax.experimental import pallas as pl
from jax.experimental.pallas import tpu as pltpu
from jax.sharding import PartitionSpec as P

MESH = pl.DeviceIdType.MESH
BF = jnp.bfloat16
F32 = jnp.float32
EPS = 1e-06


def dot(a, b):
    return jnp.dot(a, b, preferred_element_type=F32)


def kernel(
    E,
    Y,
    CAP,
    mrows_hbm,
    mgain,
    win_hbm,
    wgi_hbm,
    wgo_hbm,
    taps,
    wmo_hbm,
    rrows_hbm,
    rgain,
    ids_ref,
    rw_ref,
    eg_hbm,
    eu_hbm,
    ed_hbm,
    mout,
    rout,
    mrows,
    mn,
    win,
    wgi,
    wgo,
    wmo,
    rrows,
    nrm,
    wgu,
    wd,
    slots,
    xs,
    xb,
    acc,
    hid,
    sbuf,
    rbuf,
    fin,
    ret,
    whi,
    wlo,
    ci,
    halo,
    ext,
    go,
    gsc,
    gpart,
    l_sem,
    wt_s,
    wt_r,
    a2a_s,
    a2a_r,
    halo_s,
    halo_r,
    g_s,
    g_r,
    ag_s,
    ag_r,
    rs_s,
    rs_r,
    ret_s,
    ret_r,
    mg_s,
    mg_r,
    md_s,
    md_r,
    rg_s,
    rg_r,
    rd_s,
    rd_r,
):
    S = Y // 2
    c = lax.axis_index("ep")
    t = lax.axis_index("tp")
    y = t // 2
    k = t % 2
    half_c = c // 2
    active = k == c % 2
    M, D = mn.shape
    T = nrm.shape[0]
    CW = D // Y
    NS = E * CAP
    R = NS // 2
    R2 = R // 2
    MH = M // 2
    MQ = M // 4
    HC = gsc.shape[0] and win.shape[1]
    partner = (c, y * 2 + 1 - k)
    ring = [(c, ((y + 1) % Y) * 2 + k), (c, ((y + Y - 1) % Y) * 2 + k)]
    sign = [1, -1]

    def remote(src, dst, ss, rs, dev):
        return pltpu.make_async_remote_copy(
            src_ref=src, dst_ref=dst, send_sem=ss, recv_sem=rs, device_id=dev, device_id_type=MESH
        )

    barrier = pltpu.get_barrier_semaphore()

    def greet(i, carry):
        pl.semaphore_signal(barrier, inc=1, device_id=((c + i) % E, t), device_id_type=MESH)
        return carry

    for dev in (partner, ring[0], ring[1]):
        pl.semaphore_signal(barrier, inc=1, device_id=dev, device_id_type=MESH)
    lax.fori_loop(1, E, greet, 0)

    FW = eg_hbm.shape[2]
    loads = [
        pltpu.make_async_copy(rrows_hbm, rrows, l_sem.at[0]),
        pltpu.make_async_copy(mrows_hbm, mrows, l_sem.at[1]),
        pltpu.make_async_copy(win_hbm, win, l_sem.at[2]),
        pltpu.make_async_copy(wgi_hbm, wgi, l_sem.at[3]),
        pltpu.make_async_copy(wgo_hbm, wgo, l_sem.at[4]),
        pltpu.make_async_copy(eg_hbm.at[0], wgu.at[:, pl.ds(0, FW)], l_sem.at[5]),
        pltpu.make_async_copy(eu_hbm.at[0], wgu.at[:, pl.ds(2 * FW, FW)], l_sem.at[6]),
        pltpu.make_async_copy(ed_hbm.at[0], wd.at[pl.ds(0, FW), :], l_sem.at[7]),
        pltpu.make_async_copy(wmo_hbm, wmo.at[pl.ds(0, HC), :], l_sem.at[8]),
    ]
    for one in loads:
        one.start()

    def slot_numbers():
        ids = ids_ref[...]
        lane = lax.broadcasted_iota(jnp.int32, (T, 128), 1)
        hit0 = lane == ids[:, 0:1]
        hit1 = lane == ids[:, 1:2]
        named = jnp.where(hit0 | hit1, 1.0, 0.0).astype(BF)
        r = lax.broadcasted_iota(jnp.int32, (T, T), 0)
        q = lax.broadcasted_iota(jnp.int32, (T, T), 1)
        lower = jnp.where(r > q, 1.0, 0.0).astype(BF)
        before = dot(lower, named)
        rank0 = jnp.sum(jnp.where(hit0, before, 0.0), axis=1, keepdims=True)
        rank1 = jnp.sum(jnp.where(hit1, before, 0.0), axis=1, keepdims=True)
        s0 = ids[:, 0:1].astype(F32) * CAP + rank0
        s1 = ids[:, 1:2].astype(F32) * CAP + rank1
        diag = r == q
        row0 = jnp.sum(jnp.where(diag, s0, 0.0), axis=0, keepdims=True)
        row1 = jnp.sum(jnp.where(diag, s1, 0.0), axis=0, keepdims=True)
        return s0, s1, row0, row1

    cols_y = pl.ds(pl.multiple_of(y * CW, CW), CW)

    def norm_routed():
        step = 32

        def body(i, carry):
            rows = pl.ds(pl.multiple_of(i * step, step), step)
            v = rrows[rows, :].astype(F32)
            scale = lax.rsqrt(jnp.mean(v * v, axis=-1, keepdims=True) + EPS)
            part = rrows[rows, cols_y].astype(F32)
            nrm[rows, :] = (part * scale * rgain[:, cols_y]).astype(BF)
            return carry

        lax.fori_loop(0, T // step, body, 0)

    loads[0].wait()

    CH = NS // 4
    EC = E // 4

    def dispatch(e):
        return remote(
            xs.at[pl.ds(pl.multiple_of(e * CAP, CAP), CAP), :],
            xb.at[y, pl.ds(pl.multiple_of(half_c * CAP, CAP), CAP), :],
            a2a_s.at[e],
            a2a_r.at[half_c],
            (e, t),
        )

    @pl.when(active)
    def _():
        s0, s1, row0, row1 = slot_numbers()
        slots[0] = jnp.broadcast_to(s0, (T, 128))
        slots[1] = jnp.broadcast_to(s1, (T, 128))
        norm_routed()
        row0 = row0.astype(jnp.int32)
        row1 = row1.astype(jnp.int32)

        def select(i, carry):
            first = ((c // EC + i) % 4) * CH
            number = lax.broadcasted_iota(jnp.int32, (CH, T), 0) + first
            pick = jnp.where((number == row0) | (number == row1), 1.0, 0.0).astype(BF)
            xs[pl.ds(pl.multiple_of(first, CH), CH), :] = dot(pick, nrm[...]).astype(BF)
            return carry

        lax.fori_loop(0, 4, select, 0)

    pl.semaphore_wait(barrier, E + 2)

    @pl.when(active)
    def _():
        def send(i, carry):
            dispatch((c + i) % E).start()
            return carry

        lax.fori_loop(1, E, send, 0)
        xb[y, pl.ds(pl.multiple_of(half_c * CAP, CAP), CAP), :] = xs[
            pl.ds(pl.multiple_of(c * CAP, CAP), CAP), :
        ]

    weights = [
        remote(eg_hbm.at[0], wgu.at[:, pl.ds(FW, FW)], wt_s.at[0], wt_r.at[0], partner),
        remote(eu_hbm.at[0], wgu.at[:, pl.ds(3 * FW, FW)], wt_s.at[1], wt_r.at[1], partner),
        remote(ed_hbm.at[0], wd.at[pl.ds(FW, FW), :], wt_s.at[2], wt_r.at[2], partner),
        remote(wmo_hbm, wmo.at[pl.ds(HC, HC), :], wt_s.at[3], wt_r.at[3], partner),
    ]
    for one in weights:
        one.start()

    for i in range(1, 5):
        loads[i].wait()

    def norm_mixer(i, carry):
        rows = pl.ds(pl.multiple_of(i * 16, 16), 16)
        v = mrows[rows, :].astype(F32)
        scale = lax.rsqrt(jnp.mean(v * v, axis=-1, keepdims=True) + EPS)
        mn[rows, :] = (v * scale * mgain[...]).astype(BF)
        return carry

    lax.fori_loop(0, M // 16, norm_mixer, 0)
    normed = mn[...]
    inner = dot(normed, win[...])
    gate_in = dot(normed, wgi[...])
    go[:, 0:HC] = dot(normed, wgo[...])
    ci[...] = jnp.zeros(ci.shape, BF)
    ci[:, 0:HC] = (gate_in * inner).astype(BF)
    send_halo = remote(ci.at[pl.ds(M - 16, 16), :], halo, halo_s, halo_r, ((c + 1) % E, t))
    send_halo.start()

    @pl.when(active)
    def _():
        for i in range(4):
            number = lax.broadcasted_iota(jnp.int32, (T, CH), 1) + i * CH
            s0 = slots[0][:, 0:1].astype(jnp.int32)
            s1 = slots[1][:, 0:1].astype(jnp.int32)
            w = jnp.where(number == s0, rw_ref[:, 0:1], 0.0) + jnp.where(
                number == s1, rw_ref[:, 1:2], 0.0
            )
            top = w.astype(BF)
            whi[:, i * CH : (i + 1) * CH] = top
            wlo[:, i * CH : (i + 1) * CH] = (w - top.astype(F32)).astype(BF)

    def ag(d, s, h):
        blk = (y + Y - sign[d] * (s - 1)) % Y
        ref = xb.at[blk, pl.ds(h * R2, R2), :]
        return remote(ref, ref, ag_s.at[d, s - 1, h], ag_r.at[d, s - 1, h], ring[d])

    def ag_wait(d, s, h):
        blk = (y + Y - sign[d] * s) % Y
        ref = xb.at[blk, pl.ds(h * R2, R2), :]
        remote(ref, ref, ag_s.at[d, s - 1, h], ag_r.at[d, s - 1, h], ring[d]).wait_recv()

    def gate_up(blk, h):
        return dot(
            xb[blk, h * R2 : (h + 1) * R2, :], wgu[pl.ds(pl.multiple_of(blk * CW, CW), CW), :]
        )

    def arrived(i, carry):
        @pl.when(jnp.logical_not(active & (i == half_c)))
        def _():
            remote(
                xs.at[pl.ds(0, CAP), :],
                xb.at[y, pl.ds(pl.multiple_of(i * CAP, CAP), CAP), :],
                a2a_s.at[0],
                a2a_r.at[i],
                (c, t),
            ).wait_recv()

        return carry

    for s in range(1, S + 2):
        for h in range(2):
            if s == 1:
                lax.fori_loop(h * (E // 4), (h + 1) * (E // 4), arrived, 0)
            for d in range(2):
                if s > 1 and (s - 1 < S or h == d):
                    ag_wait(d, s - 1, h)
                if s <= S and (s < S or h == d):
                    ag(d, s, h).start()
            if s == 1 and h == 0:
                loads[5].wait()
                loads[6].wait()
                weights[0].wait_recv()
                weights[1].wait_recv()
            if s == 1:
                acc[h] = gate_up(y, h)
            elif s <= S:
                acc[h] += gate_up((y + s - 1) % Y, h) + gate_up((y + Y - s + 1) % Y, h)
            else:
                both = acc[h] + gate_up((y + S) % Y, h)
                g = both[:, 0 : 2 * FW]
                hid[h] = (g / (1.0 + jnp.exp(-g)) * both[:, 2 * FW :]).astype(BF)
        if s == 1:
            send_halo.wait_recv()
            ext[0:16, :] = jnp.where(c > 0, halo[...].astype(F32), 0.0)
            ext[16:, :] = ci[...].astype(F32)
            conv = taps[0:1, :] * ext[14 : 14 + M, 0:HC]
            conv = conv + taps[1:2, :] * ext[15 : 15 + M, 0:HC]
            conv = conv + taps[2:3, :] * ext[16 : 16 + M, 0:HC]
            gsc[...] = jnp.zeros(gsc.shape, BF)
            gsc[:, 0:HC] = (go[:, 0:HC] * conv).astype(BF)
            send_g = remote(
                gsc.at[pl.ds(pl.multiple_of((1 - k) * MH, MH), MH), :], gpart, g_s, g_r, partner
            )
            send_g.start()

    loads[7].wait()
    loads[8].wait()
    weights[2].wait_recv()
    weights[3].wait_recv()
    send_g.wait_recv()

    def partial(h, dest):
        cols = pl.ds(pl.multiple_of(dest * CW, CW), CW)
        mine = gsc[pl.ds(pl.multiple_of(k * MH + h * MQ, MQ), MQ), :]
        other = gpart[h * MQ : (h + 1) * MQ, :]
        return dot(hid[h], wd[:, cols]), dot(mine[:, 0:HC], wmo[0:HC, cols]) + dot(
            other[:, 0:HC], wmo[HC:, cols]
        )

    def rs(d, s, h):
        return remote(
            sbuf.at[d, s - 1, h], rbuf.at[d, s - 1, h], rs_s.at[d, s - 1, h], rs_r.at[d, s - 1, h], ring[d]
        )

    for s in range(1, S + 1):
        for h in range(2):
            for d in range(2):
                if s == 1 and h != d:
                    continue
                a, b = partial(h, (y + Y + sign[d] * (S + 1 - s)) % Y)
                if s > 2 or (s == 2 and h == d):
                    rs(d, s - 1, h).wait_recv()
                    a = a + rbuf[d, s - 2, h, 0:R2, :].astype(F32)
                    b = b + rbuf[d, s - 2, h, R2:, :].astype(F32)
                sbuf[d, s - 1, h, 0:R2, :] = a.astype(BF)
                sbuf[d, s - 1, h, R2:, :] = b.astype(BF)
                rs(d, s, h).start()

    def giving(i):
        return remote(
            fin.at[pl.ds(pl.multiple_of(i * CAP, CAP), CAP), :],
            ret.at[pl.ds(pl.multiple_of(c * CAP, CAP), CAP), :],
            ret_s.at[i],
            ret_r.at[c],
            (2 * i + k, t),
        )

    def give(i, carry):
        @pl.when(2 * i + k != c)
        def _():
            giving(i).start()

        return carry

    for h in range(2):
        a, b = partial(h, y)
        for d in range(2):
            rs(d, S, h).wait_recv()
            a = a + rbuf[d, S - 1, h, 0:R2, :].astype(F32)
            b = b + rbuf[d, S - 1, h, R2:, :].astype(F32)
        fin[h * R2 : (h + 1) * R2, :] = a.astype(BF)
        mout[pl.ds(pl.multiple_of(k * MH + h * MQ, MQ), MQ), cols_y] = b.astype(BF)
        lax.fori_loop(h * (E // 4), (h + 1) * (E // 4), give, 0)

    def block(rel):
        return pl.ds(pl.multiple_of(((y + Y + rel) % Y) * CW, CW), CW)

    def mixer_piece(core, rel, h):
        if h is None:
            return mout.at[pl.ds(pl.multiple_of(core * MH, MH), MH), block(rel)]
        return mout.at[pl.ds(pl.multiple_of(core * MH + h * MQ, MQ), MQ), block(rel)]

    def mg(d, s, incoming):
        rel = -sign[d] * (s if incoming else s - 1)
        ref = mixer_piece(k, rel, None if s < S else d)
        return remote(ref, ref, mg_s.at[d, s - 1], mg_r.at[d, s - 1], ring[d])

    def md(i, core, rel, h):
        ref = mixer_piece(core, rel, h)
        return remote(ref, ref, md_s.at[i], md_r.at[i], partner)

    pieces = [(0, None)]
    for s in range(1, S):
        pieces += [(-s, None), (s, None)]
    pieces += [(S, 0), (S, 1)]

    mg(0, 1, False).start()
    mg(1, 1, False).start()
    md(0, k, *pieces[0]).start()

    @pl.when(active)
    def _():
        ret[pl.ds(pl.multiple_of(c * CAP, CAP), CAP), :] = fin[
            pl.ds(pl.multiple_of(half_c * CAP, CAP), CAP), :
        ]

    for s in range(1, S + 1):
        for d in range(2):
            mg(d, s, True).wait_recv()
            if s < S:
                mg(d, s + 1, False).start()
            i = 1 + (s - 1) * 2 + d
            md(i, k, *pieces[i]).start()

    def routed_piece(rel, h):
        return rout.at[pl.ds(h * (T // 2), T // 2), block(rel)]

    def rg(d, s, h, incoming):
        ref = routed_piece(-sign[d] * (s if incoming else s - 1), h)
        return remote(ref, ref, rg_s.at[d, s - 1, h], rg_r.at[d, s - 1, h], ring[d])

    rels = [0]
    for s in range(1, S):
        rels += [-s, s]
    rels += [S]

    def rd(i, h):
        ref = routed_piece(rels[i], h)
        return remote(ref, ref, rd_s.at[i, h], rd_r.at[i, h], partner)

    @pl.when(active)
    def _():
        def back(i, carry):
            e = (c + i) % E
            remote(
                fin.at[pl.ds(0, CAP), :],
                ret.at[pl.ds(pl.multiple_of(e * CAP, CAP), CAP), :],
                ret_s.at[0],
                ret_r.at[e],
                (c, t),
            ).wait_recv()
            return carry

        lax.fori_loop(1, E, back, 0)
        for h in range(2):
            rows = slice(h * (T // 2), (h + 1) * (T // 2))
            total = dot(whi[rows, :], ret[...]) + dot(wlo[rows, :], ret[...])
            rout[rows, cols_y] = total.astype(BF)
            for d in range(2):
                rg(d, 1, h, False).start()
            rd(0, h).start()
        for s in range(1, S + 1):
            for h in range(2):
                for d in range(2):
                    if s == S and h != d:
                        continue
                    rg(d, s, h, True).wait_recv()
                    if s + 1 < S or (s + 1 == S and h == d):
                        rg(d, s + 1, h, False).start()
                    rd(1 + (s - 1) * 2 + (d if s < S else 0), h).start()

    for i, piece in enumerate(pieces):
        md(i, k, *piece).wait_send()
        md(i, 1 - k, *piece).wait_recv()
    for one in weights:
        one.wait_send()
    send_halo.wait_send()
    send_g.wait_send()
    for s in range(1, S + 1):
        for d in range(2):
            mg(d, s, False).wait_send()
            for h in range(2):
                if s < S or h == d:
                    ag(d, s, h).wait_send()
                if s > 1 or h == d:
                    rs(d, s, h).wait_send()

    def gave(i, carry):
        @pl.when(2 * i + k != c)
        def _():
            giving(i).wait_send()

        return carry

    lax.fori_loop(0, E // 2, gave, 0)

    @pl.when(active)
    def _():
        def sent(i, carry):
            dispatch((c + i) % E).wait_send()
            return carry

        lax.fori_loop(1, E, sent, 0)
        for s in range(1, S + 1):
            for h in range(2):
                for d in range(2):
                    if s < S or h == d:
                        rg(d, s, h, False).wait_send()
        for i in range(len(rels)):
            for h in range(2):
                rd(i, h).wait_send()

    @pl.when(jnp.logical_not(active))
    def _():
        for i in range(len(rels)):
            for h in range(2):
                rd(i, h).wait_recv()


def on_device(E, Y, mrows, mgain, win, wgi, wgo, taps, wmo, rrows, rgain, ids, rw, eg, eu, ed):
    M, D = mrows.shape
    T = rrows.shape[0]
    HC = win.shape[1]
    FW = eg.shape[2]
    CW = D // Y
    S = Y // 2
    CAP = 2 * T * ids.shape[1] // E
    R = E * CAP // 2
    R2 = R // 2
    MQ = M // 4
    VM = pl.BlockSpec(memory_space=pltpu.VMEM)
    HB = pl.BlockSpec(memory_space=pl.ANY)
    DS = pltpu.SemaphoreType.DMA
    n_pieces = 2 * S + 1
    return pl.pallas_call(
        functools.partial(kernel, E, Y, CAP),
        out_shape=(
            jax.ShapeDtypeStruct((M, D), BF),
            jax.ShapeDtypeStruct((T, D), BF),
        ),
        in_specs=[HB, VM, HB, HB, HB, VM, HB, HB, VM, VM, VM, HB, HB, HB],
        out_specs=(VM, VM),
        scratch_shapes=[
            pltpu.VMEM((M, D), BF),
            pltpu.VMEM((M, D), BF),
            pltpu.VMEM((D, HC), BF),
            pltpu.VMEM((D, HC), BF),
            pltpu.VMEM((D, HC), BF),
            pltpu.VMEM((2 * HC, D), BF),
            pltpu.VMEM((T, D), BF),
            pltpu.VMEM((T, CW), BF),
            pltpu.VMEM((D, 4 * FW), BF),
            pltpu.VMEM((2 * FW, D), BF),
            pltpu.VMEM((2, T, 128), F32),
            pltpu.VMEM((E * CAP, CW), BF),
            pltpu.VMEM((Y, R, CW), BF),
            pltpu.VMEM((2, R2, 4 * FW), F32),
            pltpu.VMEM((2, R2, 2 * FW), BF),
            pltpu.VMEM((2, S, 2, R2 + MQ, CW), BF),
            pltpu.VMEM((2, S, 2, R2 + MQ, CW), BF),
            pltpu.VMEM((R, CW), BF),
            pltpu.VMEM((E * CAP, CW), BF),
            pltpu.VMEM((T, E * CAP), BF),
            pltpu.VMEM((T, E * CAP), BF),
            pltpu.VMEM((M, 128), BF),
            pltpu.VMEM((16, 128), BF),
            pltpu.VMEM((M + 16, 128), F32),
            pltpu.VMEM((M, 128), F32),
            pltpu.VMEM((M, 128), BF),
            pltpu.VMEM((M // 2, 128), BF),
            DS((9,)),
            DS((4,)),
            DS((4,)),
            DS((E,)),
            DS((E // 2,)),
            DS,
            DS,
            DS,
            DS,
            DS((2, S, 2)),
            DS((2, S, 2)),
            DS((2, S, 2)),
            DS((2, S, 2)),
            DS((E // 2,)),
            DS((E,)),
            DS((2, S)),
            DS((2, S)),
            DS((n_pieces,)),
            DS((n_pieces,)),
            DS((2, S, 2)),
            DS((2, S, 2)),
            DS((2 * S, 2)),
            DS((2 * S, 2)),
        ],
        compiler_params=pltpu.CompilerParams(collective_id=0, has_side_effects=True),
    )(
        mrows,
        mgain.reshape(1, D),
        win,
        wgi,
        wgo,
        taps,
        wmo,
        rrows,
        rgain.reshape(1, D),
        ids,
        rw,
        eg,
        eu,
        ed,
    )


def solution(mesh):
    E = mesh.shape["ep"]
    Y = mesh.shape["tp"] // 2
    return jax.shard_map(
        functools.partial(on_device, E, Y),
        mesh=mesh,
        in_specs=(
            P("ep", None),
            P(),
            P(None, "tp"),
            P(None, "tp"),
            P(None, "tp"),
            P(None, "tp"),
            P("tp", None),
            P("ep", None),
            P(),
            P("ep", None),
            P("ep", None),
            P("ep", None, "tp"),
            P("ep", None, "tp"),
            P("ep", "tp", None),
        ),
        out_specs=(P("ep", None), P("ep", None)),
        check_vma=False,
    )
```

```python
import functools

import jax
import jax.numpy as jnp
from jax import lax
from jax.experimental import pallas as pl
from jax.experimental.pallas import tpu as pltpu
from jax.sharding import PartitionSpec as P

MESH = pl.DeviceIdType.MESH
BF = jnp.bfloat16
F32 = jnp.float32
EPS = 1e-06


def dot(a, b):
    return jnp.dot(a, b, preferred_element_type=F32)


def dot_t(a, b):
    return lax.dot_general(a, b, (((1,), (1,)), ((), ())), preferred_element_type=F32)


def kernel(
    E,
    Y,
    X,
    NW,
    CAP,
    mrows_hbm,
    mgain_hbm,
    win_hbm,
    wgi_hbm,
    wgo_hbm,
    taps_hbm,
    wmo_hbm,
    rrows_hbm,
    rgain_hbm,
    ids_hbm,
    rw_hbm,
    eg_hbm,
    eu_hbm,
    ed_hbm,
    mout,
    rout,
    mgain,
    taps,
    rgain,
    ids_ref,
    rw_ref,
    mrows,
    mn,
    win,
    wgi,
    wgo,
    wmo,
    rrows,
    nrm,
    nfull,
    rscale,
    wgu,
    wd,
    slots,
    slotrow,
    xs,
    xsn,
    xb,
    xn,
    acc,
    hid,
    sbuf,
    rbuf,
    fin,
    ret,
    whi,
    wlo,
    ci,
    halo,
    ext,
    go,
    gsc,
    gpart,
    l_sem,
    wt_s,
    wt_r,
    a2a_s,
    a2a_r,
    halo_s,
    halo_r,
    g_s,
    g_r,
    ag_s,
    ag_r,
    rs_s,
    rs_r,
    ret_s,
    ret_r,
    mg_s,
    mg_r,
    md_s,
    md_r,
    rg_s,
    rg_r,
    rd_s,
    rd_r,
):
    S = Y // 2
    c = lax.axis_index("ep")
    t = lax.axis_index("tp")
    y = t // 2
    k = t % 2
    half_c = c // 2
    z = c // X
    x = c % X
    active = k == c % 2
    M, D = mn.shape
    T = nrm.shape[0]
    CW = D // Y
    NS = E * CAP
    R = NS // 2
    R2 = R // 2
    Z = E // X
    NN = 2 * NW + 1
    NF = Z - NN
    PS = X * CAP
    NP = NN * X // 2
    FP = NF * X // 2
    RN = NP * CAP
    RF = FP * CAP
    RF2 = RF // 2
    MH = M // 2
    MQ = M // 4
    HC = win.shape[0]
    EP = -(-E // 16) * 16
    partner = (c, y * 2 + 1 - k)
    ring = [(c, ((y + 1) % Y) * 2 + k), (c, ((y + Y - 1) % Y) * 2 + k)]
    sign = [1, -1]

    def remote(src, dst, ss, rs, dev):
        return pltpu.make_async_remote_copy(
            src_ref=src, dst_ref=dst, send_sem=ss, recv_sem=rs, device_id=dev, device_id_type=MESH
        )

    barrier = pltpu.get_barrier_semaphore()

    def greet(i, carry):
        pl.semaphore_signal(barrier, inc=1, device_id=((c + i) % E, t), device_id_type=MESH)
        return carry

    for dev in (partner, ring[0], ring[1]):
        pl.semaphore_signal(barrier, inc=1, device_id=dev, device_id_type=MESH)
    lax.fori_loop(1, E, greet, 0)

    FW = eg_hbm.shape[2]
    loads = [
        pltpu.make_async_copy(rrows_hbm, rrows, l_sem.at[0]),
        pltpu.make_async_copy(mrows_hbm, mrows, l_sem.at[1]),
        pltpu.make_async_copy(win_hbm, win, l_sem.at[2]),
        pltpu.make_async_copy(wgi_hbm, wgi, l_sem.at[3]),
        pltpu.make_async_copy(wgo_hbm, wgo, l_sem.at[4]),
        pltpu.make_async_copy(eg_hbm.at[0], wgu.at[:, pl.ds(0, FW)], l_sem.at[5]),
        pltpu.make_async_copy(eu_hbm.at[0], wgu.at[:, pl.ds(2 * FW, FW)], l_sem.at[6]),
        pltpu.make_async_copy(ed_hbm.at[0], wd.at[pl.ds(0, FW), :], l_sem.at[7]),
        pltpu.make_async_copy(wmo_hbm, wmo.at[pl.ds(0, HC), :], l_sem.at[8]),
        pltpu.make_async_copy(ids_hbm, ids_ref, l_sem.at[9]),
        pltpu.make_async_copy(rw_hbm, rw_ref, l_sem.at[10]),
        pltpu.make_async_copy(rgain_hbm, rgain, l_sem.at[11]),
        pltpu.make_async_copy(mgain_hbm, mgain, l_sem.at[12]),
        pltpu.make_async_copy(taps_hbm, taps, l_sem.at[13]),
    ]
    for i in (9, 10, 0, 11, 1, 12, 2, 3, 4, 13, 5, 6, 7, 8):
        loads[i].start()

    def slot_numbers():
        ids = ids_ref[...]
        expert = lax.broadcasted_iota(jnp.int32, (EP, T), 0)
        hit0 = expert == ids[0:1, :]
        hit1 = expert == ids[1:2, :]
        named = jnp.where(hit0 | hit1, 1.0, 0.0).astype(BF)
        r = lax.broadcasted_iota(jnp.int32, (T, T), 0)
        q = lax.broadcasted_iota(jnp.int32, (T, T), 1)
        upper = jnp.where(r < q, 1.0, 0.0).astype(BF)
        before = dot(named, upper)
        row0 = ids[0:1, :].astype(F32) * CAP + jnp.sum(
            jnp.where(hit0, before, 0.0), axis=0, keepdims=True
        )
        row1 = ids[1:2, :].astype(F32) * CAP + jnp.sum(
            jnp.where(hit1, before, 0.0), axis=0, keepdims=True
        )
        diag = r == q

        def column(row):
            one = jnp.sum(jnp.where(diag, row, 0.0), axis=1, keepdims=True)
            return jnp.broadcast_to(one, (T, 128))

        columns = (row0, row1, rw_ref[0:1, :], rw_ref[1:2, :])
        for i, row in enumerate(columns):
            slots[i] = column(row)
        return row0, row1

    cols_y = pl.ds(pl.multiple_of(y * CW, CW), CW)

    def norm_routed():
        step = 32

        def body(i, carry):
            rows = pl.ds(pl.multiple_of(i * step, step), step)
            v = rrows[rows, :].astype(F32)
            scale = lax.rsqrt(jnp.mean(v * v, axis=-1, keepdims=True) + EPS)
            rscale[rows, :] = jnp.broadcast_to(scale, (step, 128))
            part = rrows[rows, cols_y].astype(F32)
            nrm[rows, :] = (part * scale * rgain[:, cols_y]).astype(BF)
            return carry

        lax.fori_loop(0, T // step, body, 0)

    loads[9].wait()
    loads[10].wait()

    CH = NS // 4

    def place(zc, xc, ze):
        return (zc - ze + Z + NW) % Z * (X // 2) + xc // 2

    def cap_rows(i):
        return pl.ds(pl.multiple_of(i * CAP, CAP), CAP)

    def far(i):
        q = i % NF
        ze = (z + NW + 1 + q) % Z
        xe = (x + i // NF) % X
        p = place(z, x, ze)
        return remote(
            xs.at[cap_rows(q * X + xe), :],
            xb.at[y, cap_rows(p - NP), :],
            a2a_s.at[q * X + xe],
            a2a_r.at[p],
            (ze * X + xe, t),
        )

    def near(i):
        n = i % NN
        ze = (z + Z - NW + n) % Z
        xe = (x + i // NN) % X
        p = place(z, x, ze)
        return remote(
            xsn.at[cap_rows(n * X + xe), :],
            xn.at[cap_rows(p), :],
            a2a_s.at[NF * X + n * X + xe],
            a2a_r.at[p],
            (ze * X + xe, t),
        )

    def pick_plane(zp):
        number = lax.broadcasted_iota(jnp.int32, (PS, T), 0) + zp * PS
        row0 = slotrow[0:1, :].astype(jnp.int32)
        row1 = slotrow[1:2, :].astype(jnp.int32)
        return jnp.where((number == row0) | (number == row1), 1.0, 0.0).astype(BF)

    def plane_rows(q):
        return pl.ds(pl.multiple_of(q * PS, PS), PS)

    @pl.when(active)
    def _():
        row0, row1 = slot_numbers()
        loads[0].wait()
        loads[11].wait()
        norm_routed()
        slotrow[0:1, :] = row0
        slotrow[1:2, :] = row1

        def select(q, carry):
            pick = pick_plane((z + NW + 1 + q) % Z)
            xs[plane_rows(q), :] = dot(pick, nrm[...]).astype(BF)
            return carry

        lax.fori_loop(0, NF, select, 0)

    @pl.when(jnp.logical_not(active))
    def _():
        loads[0].wait()
        loads[11].wait()

    pl.semaphore_wait(barrier, E + 2)

    @pl.when(active)
    def _():
        def send_far(i, carry):
            far(i).start()
            return carry

        lax.fori_loop(0, NF * X, send_far, 0)

        def norm_full(i, carry):
            rows = pl.ds(pl.multiple_of(i * 16, 16), 16)
            v = rrows[rows, :].astype(F32)
            nfull[rows, :] = (v * rscale[rows, 0:1] * rgain[...]).astype(BF)
            return carry

        lax.fori_loop(0, T // 16, norm_full, 0)

        def select_near(n, carry):
            pick = pick_plane((z + Z - NW + n) % Z)
            xsn[plane_rows(n), :] = dot(pick, nfull[...]).astype(BF)
            return carry

        lax.fori_loop(0, NN, select_near, 0)

        def send_near(i, carry):
            @pl.when(i != NW)
            def _():
                near(i).start()

            return carry

        lax.fori_loop(0, NN * X, send_near, 0)
        xn[cap_rows(place(z, x, z)), :] = xsn[cap_rows(NW * X + x), :]

    weights = [
        remote(eg_hbm.at[0], wgu.at[:, pl.ds(FW, FW)], wt_s.at[0], wt_r.at[0], partner),
        remote(eu_hbm.at[0], wgu.at[:, pl.ds(3 * FW, FW)], wt_s.at[1], wt_r.at[1], partner),
        remote(ed_hbm.at[0], wd.at[pl.ds(FW, FW), :], wt_s.at[2], wt_r.at[2], partner),
        remote(wmo_hbm, wmo.at[pl.ds(HC, HC), :], wt_s.at[3], wt_r.at[3], partner),
    ]
    for one in weights:
        one.start()

    for i in (1, 2, 3, 4, 12, 13):
        loads[i].wait()

    def norm_mixer(i, carry):
        rows = pl.ds(pl.multiple_of(i * 16, 16), 16)
        v = mrows[rows, :].astype(F32)
        scale = lax.rsqrt(jnp.mean(v * v, axis=-1, keepdims=True) + EPS)
        mn[rows, :] = (v * scale * mgain[...]).astype(BF)
        return carry

    lax.fori_loop(0, M // 16, norm_mixer, 0)
    normed = mn[...]
    inner = dot_t(normed, win[...])
    gate_in = dot_t(normed, wgi[...])
    go[:, 0:HC] = dot_t(normed, wgo[...])
    ci[...] = jnp.zeros(ci.shape, BF)
    ci[:, 0:HC] = (gate_in * inner).astype(BF)
    send_halo = remote(ci.at[pl.ds(M - 16, 16), :], halo, halo_s, halo_r, ((c + 1) % E, t))
    send_halo.start()

    @pl.when(active)
    def _():
        for i in range(4):
            number = lax.broadcasted_iota(jnp.int32, (T, CH), 1) + i * CH
            s0 = slots[0][:, 0:1].astype(jnp.int32)
            s1 = slots[1][:, 0:1].astype(jnp.int32)
            w = jnp.where(number == s0, slots[2][:, 0:1], 0.0) + jnp.where(
                number == s1, slots[3][:, 0:1], 0.0
            )
            top = w.astype(BF)
            whi[:, i * CH : (i + 1) * CH] = top
            wlo[:, i * CH : (i + 1) * CH] = (w - top.astype(F32)).astype(BF)

    def ag(d, s, h):
        blk = (y + Y - sign[d] * (s - 1)) % Y
        ref = xb.at[blk, pl.ds(h * RF2, RF2), :]
        return remote(ref, ref, ag_s.at[d, s - 1, h], ag_r.at[d, s - 1, h], ring[d])

    def ag_wait(d, s, h):
        blk = (y + Y - sign[d] * s) % Y
        ref = xb.at[blk, pl.ds(h * RF2, RF2), :]
        remote(ref, ref, ag_s.at[d, s - 1, h], ag_r.at[d, s - 1, h], ring[d]).wait_recv()

    def gate_up(blk, h):
        return dot(
            xb[blk, h * RF2 : (h + 1) * RF2, :], wgu[pl.ds(pl.multiple_of(blk * CW, CW), CW), :]
        )

    def far_arrived(i, carry):
        remote(
            xs.at[pl.ds(0, CAP), :],
            xb.at[y, cap_rows(i), :],
            a2a_s.at[0],
            a2a_r.at[NP + i],
            (c, t),
        ).wait_recv()
        return carry

    def near_arrived(i, carry):
        @pl.when(jnp.logical_not(active & (i == place(z, x, z))))
        def _():
            remote(
                xsn.at[pl.ds(0, CAP), :], xn.at[cap_rows(i), :], a2a_s.at[0], a2a_r.at[i], (c, t)
            ).wait_recv()

        return carry

    def finish(both, rows):
        g = both[:, 0 : 2 * FW]
        hid[rows, :] = (g / (1.0 + jnp.exp(-g)) * both[:, 2 * FW :]).astype(BF)

    for s in range(1, S + 2):
        for h in range(2):
            if s == 1:
                lax.fori_loop(h * (FP // 2), (h + 1) * (FP // 2), far_arrived, 0)
            for d in range(2):
                if s > 1 and (s - 1 < S or h == d):
                    ag_wait(d, s - 1, h)
                if s <= S and (s < S or h == d):
                    ag(d, s, h).start()
            if s == 1 and h == 0:
                loads[5].wait()
                loads[6].wait()
                weights[0].wait_recv()
                weights[1].wait_recv()
            if s == 1:
                acc[h] = gate_up(y, h)
            elif s <= S:
                acc[h] += gate_up((y + s - 1) % Y, h) + gate_up((y + Y - s + 1) % Y, h)
            else:
                finish(
                    acc[h] + gate_up((y + S) % Y, h), slice(RN + h * RF2, RN + (h + 1) * RF2)
                )
        if s == S:
            lax.fori_loop(0, NP, near_arrived, 0)
            finish(dot(xn[...], wgu[...]), slice(0, RN))
        if s == 2:
            send_halo.wait_recv()
            ext[0:16, :] = jnp.where(c > 0, halo[...].astype(F32), 0.0)
            ext[16:, :] = ci[...].astype(F32)
            conv = taps[0:1, :] * ext[14 : 14 + M, 0:HC]
            conv = conv + taps[1:2, :] * ext[15 : 15 + M, 0:HC]
            conv = conv + taps[2:3, :] * ext[16 : 16 + M, 0:HC]
            gsc[...] = jnp.zeros(gsc.shape, BF)
            gsc[:, 0:HC] = (go[:, 0:HC] * conv).astype(BF)
            send_g = remote(
                gsc.at[pl.ds(pl.multiple_of((1 - k) * MH, MH), MH), :], gpart, g_s, g_r, partner
            )
            send_g.start()

    loads[7].wait()
    loads[8].wait()
    weights[2].wait_recv()
    weights[3].wait_recv()
    send_g.wait_recv()

    def partial(h, dest):
        cols = pl.ds(pl.multiple_of(dest * CW, CW), CW)
        mine = gsc[pl.ds(pl.multiple_of(k * MH + h * MQ, MQ), MQ), :]
        other = gpart[h * MQ : (h + 1) * MQ, :]
        return dot(hid[h * R2 : (h + 1) * R2, :], wd[:, cols]), dot(mine[:, 0:HC], wmo[0:HC, cols]) + dot(
            other[:, 0:HC], wmo[HC:, cols]
        )

    def rs(d, s, h):
        return remote(
            sbuf.at[d, s - 1, h], rbuf.at[d, s - 1, h], rs_s.at[d, s - 1, h], rs_r.at[d, s - 1, h], ring[d]
        )

    order = [(1, 0, 0), (1, 1, 1)]
    for s in range(2, S + 1):
        order += [(s, 1, 0), (s, 0, 1), (s, 0, 0), (s, 1, 1)]
    for s, h, d in order:
        a, b = partial(h, (y + Y + sign[d] * (S + 1 - s)) % Y)
        if s > 2 or (s == 2 and h == d):
            rs(d, s - 1, h).wait_recv()
            a = a + rbuf[d, s - 2, h, 0:R2, :].astype(F32)
            b = b + rbuf[d, s - 2, h, R2:, :].astype(F32)
        sbuf[d, s - 1, h, 0:R2, :] = a.astype(BF)
        sbuf[d, s - 1, h, R2:, :] = b.astype(BF)
        rs(d, s, h).start()

    def target(i):
        zc = (z + Z - NW + i // (X // 2)) % Z
        return zc * X + i % (X // 2) * 2 + k

    def giving(i):
        return remote(
            fin.at[cap_rows(i), :], ret.at[cap_rows(c), :], ret_s.at[i], ret_r.at[c], (target(i), t)
        )

    def give(i, carry):
        @pl.when(target(i) != c)
        def _():
            giving(i).start()

        return carry

    for h in range(2):
        a, b = partial(h, y)
        for d in (1 - h, h):
            rs(d, S, h).wait_recv()
            a = a + rbuf[d, S - 1, h, 0:R2, :].astype(F32)
            b = b + rbuf[d, S - 1, h, R2:, :].astype(F32)
        fin[h * R2 : (h + 1) * R2, :] = a.astype(BF)
        mout[pl.ds(pl.multiple_of(k * MH + h * MQ, MQ), MQ), cols_y] = b.astype(BF)
        lax.fori_loop(h * (E // 4), (h + 1) * (E // 4), give, 0)

    def block(rel):
        return pl.ds(pl.multiple_of(((y + Y + rel) % Y) * CW, CW), CW)

    def mixer_piece(core, rel):
        return mout.at[pl.ds(pl.multiple_of(core * MH, MH), MH), block(rel)]

    def mg(i, rel):
        ref = mixer_piece(k, rel)
        return remote(ref, ref, mg_s.at[i], mg_r.at[i], (c, ((y + i) % Y) * 2 + k))

    def md(i, core):
        ref = mixer_piece(core, -i)
        return remote(ref, ref, md_s.at[i], md_r.at[i], partner)

    for i in range(1, S):
        mg(i, 0).start()
        mg(Y - i, 0).start()
    mg(S, 0).start()
    md(0, k).start()

    @pl.when(active)
    def _():
        ret[cap_rows(c), :] = fin[cap_rows(place(z, x, z)), :]

    def pass_mixer():
        for i in range(1, Y):
            mg(i, -i).wait_recv()
            md(i, k).start()

    def routed_piece(rel, h):
        return rout.at[pl.ds(h * (T // 2), T // 2), block(rel)]

    def pieces(j):
        return [(d, h) for h in range(2) for d in range(2) if j < S or h == d]

    def rg(d, j, h, incoming):
        if incoming:
            ref = routed_piece(-sign[d] * j, h)
        else:
            ref = routed_piece(0 if j <= 2 else -sign[d] * 2, h)
        dev = (c, ((y + Y + sign[d] * (j if j <= 2 else j - 2)) % Y) * 2 + k)
        return remote(ref, ref, rg_s.at[d, j - 1, h], rg_r.at[d, j - 1, h], dev)

    def rd(d, j, h):
        i = 0 if j == 0 else 1 + (j - 1) * 2 + (d if j < S else 0)
        ref = routed_piece(-sign[d] * j, h)
        return remote(ref, ref, rd_s.at[i, h], rd_r.at[i, h], partner)

    shared = [(0, 0, 0), (0, 0, 1)]
    for j in range(1, S + 1):
        shared += [(d, j, h) for d, h in pieces(j)]

    @pl.when(active)
    def _():
        def back(i, carry):
            e = (c + i) % E
            remote(
                fin.at[pl.ds(0, CAP), :],
                ret.at[pl.ds(pl.multiple_of(e * CAP, CAP), CAP), :],
                ret_s.at[0],
                ret_r.at[e],
                (c, t),
            ).wait_recv()
            return carry

        lax.fori_loop(1, E, back, 0)
        for h in range(2):
            rows = slice(h * (T // 2), (h + 1) * (T // 2))
            total = dot(whi[rows, :], ret[...]) + dot(wlo[rows, :], ret[...])
            rout[rows, cols_y] = total.astype(BF)
            for d in range(2):
                if 2 < S or h == d:
                    rg(d, 2, h, False).start()
            rd(0, 0, h).start()
        for d, h in pieces(1):
            rg(d, 1, h, False).start()
        pass_mixer()
        for d, h in pieces(2):
            rg(d, 2, h, True).wait_recv()
            for j in range(S, 2, -1):
                if (d, h) in pieces(j):
                    rg(d, j, h, False).start()
            rd(d, 2, h).start()
        for j in [1] + list(range(3, S + 1)):
            for d, h in pieces(j):
                rg(d, j, h, True).wait_recv()
                rd(d, j, h).start()

    @pl.when(jnp.logical_not(active))
    def _():
        pass_mixer()

    for i in range(Y):
        md(i, k).wait_send()
        md(i, 1 - k).wait_recv()
        if i > 0:
            mg(i, 0).wait_send()
    for one in weights:
        one.wait_send()
    send_halo.wait_send()
    send_g.wait_send()
    for s in range(1, S + 1):
        for d in range(2):
            for h in range(2):
                if s < S or h == d:
                    ag(d, s, h).wait_send()
                if s > 1 or h == d:
                    rs(d, s, h).wait_send()

    def gave(i, carry):
        @pl.when(target(i) != c)
        def _():
            giving(i).wait_send()

        return carry

    lax.fori_loop(0, E // 2, gave, 0)

    @pl.when(active)
    def _():
        def sent_far(i, carry):
            far(i).wait_send()
            return carry

        def sent_near(i, carry):
            @pl.when(i != NW)
            def _():
                near(i).wait_send()

            return carry

        lax.fori_loop(0, NF * X, sent_far, 0)
        lax.fori_loop(0, NN * X, sent_near, 0)
        for j in range(1, S + 1):
            for d, h in pieces(j):
                rg(d, j, h, False).wait_send()
        for one in shared:
            rd(*one).wait_send()

    @pl.when(jnp.logical_not(active))
    def _():
        for one in shared:
            rd(*one).wait_recv()


def on_device(E, Y, mrows, mgain, win, wgi, wgo, taps, wmo, rrows, rgain, ids, rw, eg, eu, ed):
    M, D = mrows.shape
    T = rrows.shape[0]
    HC = win.shape[1]
    FW = eg.shape[2]
    CW = D // Y
    S = Y // 2
    CAP = 2 * T * ids.shape[1] // E
    X = 4
    NW = 1 if E // X > 3 else 0
    RN = (2 * NW + 1) * (X // 2) * CAP
    R = E * CAP // 2
    R2 = R // 2
    MQ = M // 4
    VM = pl.BlockSpec(memory_space=pltpu.VMEM)
    HB = pl.BlockSpec(memory_space=pl.ANY)
    DS = pltpu.SemaphoreType.DMA
    return pl.pallas_call(
        functools.partial(kernel, E, Y, X, NW, CAP),
        out_shape=(pltpu.VMEM((M, D), BF), pltpu.VMEM((T, D), BF)),
        in_specs=[HB] * 14,
        out_specs=(VM, VM),
        scratch_shapes=[
            pltpu.VMEM((1, D), F32),
            pltpu.VMEM(taps.shape, F32),
            pltpu.VMEM((1, D), F32),
            pltpu.VMEM((2, T), jnp.int32),
            pltpu.VMEM((2, T), F32),
            pltpu.VMEM((M, D), BF),
            pltpu.VMEM((M, D), BF),
            pltpu.VMEM((HC, D), BF),
            pltpu.VMEM((HC, D), BF),
            pltpu.VMEM((HC, D), BF),
            pltpu.VMEM((2 * HC, D), BF),
            pltpu.VMEM((T, D), BF),
            pltpu.VMEM((T, CW), BF),
            pltpu.VMEM((T, D), BF),
            pltpu.VMEM((T, 128), F32),
            pltpu.VMEM((D, 4 * FW), BF),
            pltpu.VMEM((2 * FW, D), BF),
            pltpu.VMEM((4, T, 128), F32),
            pltpu.VMEM((8, T), F32),
            pltpu.VMEM(((R - RN) * 2, CW), BF),
            pltpu.VMEM((2 * RN, D), BF),
            pltpu.VMEM((Y, R - RN, CW), BF),
            pltpu.VMEM((RN, D), BF),
            pltpu.VMEM((2, (R - RN) // 2, 4 * FW), F32),
            pltpu.VMEM((R, 2 * FW), BF),
            pltpu.VMEM((2, S, 2, R2 + MQ, CW), BF),
            pltpu.VMEM((2, S, 2, R2 + MQ, CW), BF),
            pltpu.VMEM((R, CW), BF),
            pltpu.VMEM((E * CAP, CW), BF),
            pltpu.VMEM((T, E * CAP), BF),
            pltpu.VMEM((T, E * CAP), BF),
            pltpu.VMEM((M, 128), BF),
            pltpu.VMEM((16, 128), BF),
            pltpu.VMEM((M + 16, 128), F32),
            pltpu.VMEM((M, 128), F32),
            pltpu.VMEM((M, 128), BF),
            pltpu.VMEM((M // 2, 128), BF),
            DS((14,)),
            DS((4,)),
            DS((4,)),
            DS((E,)),
            DS((E // 2,)),
            DS,
            DS,
            DS,
            DS,
            DS((2, S, 2)),
            DS((2, S, 2)),
            DS((2, S, 2)),
            DS((2, S, 2)),
            DS((E // 2,)),
            DS((E,)),
            DS((Y,)),
            DS((Y,)),
            DS((Y,)),
            DS((Y,)),
            DS((2, S, 2)),
            DS((2, S, 2)),
            DS((2 * S, 2)),
            DS((2 * S, 2)),
        ],
        compiler_params=pltpu.CompilerParams(collective_id=0, has_side_effects=True),
    )(
        mrows,
        mgain.reshape(1, D),
        win.T,
        wgi.T,
        wgo.T,
        taps,
        wmo,
        rrows,
        rgain.reshape(1, D),
        ids.T,
        rw.T,
        eg,
        eu,
        ed,
    )


def solution(mesh):
    E = mesh.shape["ep"]
    Y = mesh.shape["tp"] // 2
    return jax.shard_map(
        functools.partial(on_device, E, Y),
        mesh=mesh,
        in_specs=(
            P("ep", None),
            P(),
            P(None, "tp"),
            P(None, "tp"),
            P(None, "tp"),
            P(None, "tp"),
            P("tp", None),
            P("ep", None),
            P(),
            P("ep", None),
            P("ep", None),
            P("ep", None, "tp"),
            P("ep", None, "tp"),
            P("ep", "tp", None),
        ),
        out_specs=(P("ep", None), P("ep", None)),
        check_vma=False,
    )
```

```python
import functools

import jax
import jax.numpy as jnp
from jax import lax
from jax.experimental import pallas as pl
from jax.experimental.pallas import tpu as pltpu
from jax.sharding import PartitionSpec as P

MESH = pl.DeviceIdType.MESH
BF = jnp.bfloat16
F32 = jnp.float32
EPS = 1e-06


def dot(a, b):
    return jnp.dot(a, b, preferred_element_type=F32)


def dot_t(a, b):
    return lax.dot_general(a, b, (((1,), (1,)), ((), ())), preferred_element_type=F32)


def kernel(
    E,
    Y,
    X,
    NW,
    CAP,
    mrows_hbm,
    mgain_hbm,
    win_hbm,
    wgi_hbm,
    wgo_hbm,
    taps_hbm,
    wmo_hbm,
    rrows_hbm,
    rgain_hbm,
    ids_hbm,
    rw_hbm,
    eg_hbm,
    eu_hbm,
    ed_hbm,
    mout,
    rout,
    mgain,
    taps,
    rgain,
    ids_ref,
    rw_ref,
    mrows,
    mn,
    win,
    wgi,
    wgo,
    wmo,
    rrows,
    nrm,
    nfull,
    rscale,
    wgu,
    wd,
    slotrow,
    xs,
    xsn,
    xb,
    xn,
    acc,
    hid,
    sbuf,
    rbuf,
    msbuf,
    mrbuf,
    fin,
    ret,
    whi,
    wlo,
    ci,
    halo,
    ext,
    go,
    gsc,
    gpart,
    l_sem,
    wt_s,
    wt_r,
    a2a_s,
    a2a_r,
    halo_s,
    halo_r,
    g_s,
    g_r,
    ag_s,
    ag_r,
    rs_s,
    rs_r,
    mx_s,
    mx_r,
    ret_s,
    ret_r,
    mg_s,
    mg_r,
    md_s,
    md_r,
    rg_s,
    rd_s,
    rd_r,
):
    S = Y // 2
    c = lax.axis_index("ep")
    t = lax.axis_index("tp")
    y = t // 2
    k = t % 2
    z = c // X
    x = c % X
    active = k == c % 2
    M, D = mn.shape
    T = nrm.shape[0]
    CW = D // Y
    NS = E * CAP
    R = NS // 2
    Z = E // X
    NN = 2 * NW + 1
    NF = Z - NN
    PS = X * CAP
    NP = NN * X // 2
    FP = NF * X // 2
    RN = NP * CAP
    RF = FP * CAP
    QS = PS // 2
    near_off = list(range(-NW, NW + 1))
    far_off = sorted(range(NW + 1, Z - NW), key=lambda g: min(g, Z - g))
    order_off = far_off + near_off
    RH = R // 2
    CH = CW // 2
    MH = M // 2
    MQ = MH // 2
    HC = win.shape[0]
    EP = -(-E // 16) * 16
    partner = (c, y * 2 + 1 - k)
    ring = [(c, ((y + 1) % Y) * 2 + k), (c, ((y + Y - 1) % Y) * 2 + k)]
    sign = [1, -1]

    def remote(src, dst, ss, rs, dev):
        return pltpu.make_async_remote_copy(
            src_ref=src, dst_ref=dst, send_sem=ss, recv_sem=rs, device_id=dev, device_id_type=MESH
        )

    def settle(ref, sem):
        pltpu.make_async_copy(ref, ref, sem).wait()

    FW = eg_hbm.shape[2]
    loads = [
        pltpu.make_async_copy(rrows_hbm, rrows, l_sem.at[0]),
        pltpu.make_async_copy(mrows_hbm, mrows, l_sem.at[1]),
        pltpu.make_async_copy(win_hbm, win, l_sem.at[2]),
        pltpu.make_async_copy(wgi_hbm, wgi, l_sem.at[3]),
        pltpu.make_async_copy(wgo_hbm, wgo, l_sem.at[4]),
        pltpu.make_async_copy(eg_hbm.at[0], wgu.at[:, pl.ds(0, FW)], l_sem.at[5]),
        pltpu.make_async_copy(eu_hbm.at[0], wgu.at[:, pl.ds(2 * FW, FW)], l_sem.at[6]),
        pltpu.make_async_copy(ed_hbm.at[0], wd.at[pl.ds(0, FW), :], l_sem.at[7]),
        pltpu.make_async_copy(wmo_hbm, wmo.at[pl.ds(0, HC), :], l_sem.at[8]),
        pltpu.make_async_copy(ids_hbm, ids_ref, l_sem.at[9]),
        pltpu.make_async_copy(rw_hbm, rw_ref, l_sem.at[10]),
        pltpu.make_async_copy(rgain_hbm, rgain, l_sem.at[11]),
        pltpu.make_async_copy(mgain_hbm, mgain, l_sem.at[12]),
        pltpu.make_async_copy(taps_hbm, taps, l_sem.at[13]),
    ]
    for i in (9, 0, 11):
        loads[i].start()

    barrier = pltpu.get_barrier_semaphore()

    def greet(i, carry):
        pl.semaphore_signal(barrier, inc=1, device_id=((c + i) % E, t), device_id_type=MESH)
        return carry

    for dev in (partner, ring[0], ring[1]):
        pl.semaphore_signal(barrier, inc=1, device_id=dev, device_id_type=MESH)
    lax.fori_loop(1, E, greet, 0)

    for i in (1, 12, 2, 3, 4, 10, 13, 5, 6, 7, 8):
        loads[i].start()

    def slot_numbers():
        ids = ids_ref[...]
        expert = lax.broadcasted_iota(jnp.int32, (EP, T), 0)
        hit0 = expert == ids[0:1, :]
        hit1 = expert == ids[1:2, :]
        named = jnp.where(hit0 | hit1, 1.0, 0.0).astype(BF)
        r = lax.broadcasted_iota(jnp.int32, (T, T), 0)
        q = lax.broadcasted_iota(jnp.int32, (T, T), 1)
        upper = jnp.where(r < q, 1.0, 0.0).astype(BF)
        before = dot(named, upper)
        row0 = ids[0:1, :].astype(F32) * CAP + jnp.sum(
            jnp.where(hit0, before, 0.0), axis=0, keepdims=True
        )
        row1 = ids[1:2, :].astype(F32) * CAP + jnp.sum(
            jnp.where(hit1, before, 0.0), axis=0, keepdims=True
        )
        return row0, row1

    def slot_columns():
        r = lax.broadcasted_iota(jnp.int32, (T, T), 0)
        q = lax.broadcasted_iota(jnp.int32, (T, T), 1)
        diag = r == q
        rows = (slotrow[0:1, :], slotrow[1:2, :], rw_ref[0:1, :], rw_ref[1:2, :])
        return [jnp.sum(jnp.where(diag, row, 0.0), axis=1, keepdims=True) for row in rows]

    cols_y = pl.ds(pl.multiple_of(y * CW, CW), CW)

    def norm_routed():
        step = 32

        def body(i, carry):
            rows = pl.ds(pl.multiple_of(i * step, step), step)
            v = rrows[rows, :].astype(F32)
            scale = lax.rsqrt(jnp.mean(v * v, axis=-1, keepdims=True) + EPS)
            rscale[rows, :] = jnp.broadcast_to(scale, (step, 128))
            part = rrows[rows, cols_y].astype(F32)
            nrm[rows, :] = (part * scale * rgain[:, cols_y]).astype(BF)
            return carry

        lax.fori_loop(0, T // step, body, 0)

    loads[9].wait()

    SC = NS // 4

    def cap_rows(i):
        return pl.ds(pl.multiple_of(i * CAP, CAP), CAP)

    def far(q, i):
        g = far_off[q]
        ze = (z + g) % Z
        xe = (x + i) % X
        row = far_off.index(Z - g) * (X // 2) + x // 2
        return remote(
            xs.at[cap_rows(q * X + xe), :],
            xb.at[y, cap_rows(row), :],
            a2a_s.at[0],
            a2a_r.at[far_off.index(Z - g)],
            (ze * X + xe, t),
        )

    def near(n, i):
        ze = (z + Z + near_off[n]) % Z
        xe = (x + i) % X
        row = (NN - 1 - n) * (X // 2) + x // 2
        return remote(
            xsn.at[cap_rows(n * X + xe), :],
            xn.at[cap_rows(row), :],
            a2a_s.at[1],
            a2a_r.at[NF],
            (ze * X + xe, t),
        )

    own_row = NW * (X // 2) + x // 2
    near_order = [n for n in range(NN) if n != NW] + [NW]

    def pick_plane(zp):
        number = lax.broadcasted_iota(jnp.int32, (PS, T), 0) + zp * PS
        row0 = slotrow[0:1, :].astype(jnp.int32)
        row1 = slotrow[1:2, :].astype(jnp.int32)
        return jnp.where((number == row0) | (number == row1), 1.0, 0.0).astype(BF)

    @pl.when(active)
    def _():
        row0, row1 = slot_numbers()
        loads[0].wait()
        loads[11].wait()
        norm_routed()
        slotrow[0:1, :] = row0
        slotrow[1:2, :] = row1

        def select(q):
            pick = pick_plane((z + far_off[q]) % Z)
            xs[q * PS : (q + 1) * PS, :] = dot(pick, nrm[...]).astype(BF)

        for q in range(NF):
            select(q)

    @pl.when(jnp.logical_not(active))
    def _():
        for i in (0, 10, 11):
            loads[i].wait()

    pl.semaphore_wait(barrier, E + 2)

    @pl.when(active)
    def _():
        for q in range(NF):

            def send_far(i, carry):
                far(q, i).start()
                return carry

            lax.fori_loop(0, X, send_far, 0)

    weights = [
        remote(eg_hbm.at[0], wgu.at[:, pl.ds(FW, FW)], wt_s.at[0], wt_r.at[0], partner),
        remote(eu_hbm.at[0], wgu.at[:, pl.ds(3 * FW, FW)], wt_s.at[1], wt_r.at[1], partner),
        remote(ed_hbm.at[0], wd.at[pl.ds(FW, FW), :], wt_s.at[2], wt_r.at[2], partner),
        remote(wmo_hbm, wmo.at[pl.ds(HC, HC), :], wt_s.at[3], wt_r.at[3], partner),
    ]
    for one in weights:
        one.start()

    for i in (1, 2, 3, 4, 12, 13):
        loads[i].wait()

    def norm_mixer(i, carry):
        rows = pl.ds(pl.multiple_of(i * 16, 16), 16)
        v = mrows[rows, :].astype(F32)
        scale = lax.rsqrt(jnp.mean(v * v, axis=-1, keepdims=True) + EPS)
        mn[rows, :] = (v * scale * mgain[...]).astype(BF)
        return carry

    lax.fori_loop(0, M // 16, norm_mixer, 0)
    normed = mn[...]
    inner = dot_t(normed, win[...])
    gate_in = dot_t(normed, wgi[...])
    go[:, 0:HC] = dot_t(normed, wgo[...])
    ci[...] = jnp.zeros(ci.shape, BF)
    ci[:, 0:HC] = (gate_in * inner).astype(BF)
    send_halo = remote(ci.at[pl.ds(M - 16, 16), :], halo, halo_s, halo_r, ((c + 1) % E, t))
    send_halo.start()

    @pl.when(active)
    def _():
        def norm_full(i, carry):
            rows = pl.ds(pl.multiple_of(i * 16, 16), 16)
            v = rrows[rows, :].astype(F32)
            nfull[rows, :] = (v * rscale[rows, 0:1] * rgain[...]).astype(BF)
            return carry

        lax.fori_loop(0, T // 16, norm_full, 0)

        for n in near_order:
            pick = pick_plane((z + Z + near_off[n]) % Z)
            xsn[n * PS : (n + 1) * PS, :] = dot(pick, nfull[...]).astype(BF)

            def send_near(i, carry):
                near(n, i).start()
                return carry

            lax.fori_loop(1 if n == NW else 0, X, send_near, 0)
        xn[cap_rows(own_row), :] = xsn[cap_rows(NW * X + x), :]

        loads[10].wait()
        s0, s1, w0, w1 = slot_columns()
        s0 = s0.astype(jnp.int32)
        s1 = s1.astype(jnp.int32)
        for i in range(4):
            number = lax.broadcasted_iota(jnp.int32, (T, SC), 1) + i * SC
            w = jnp.where(number == s0, w0, 0.0) + jnp.where(number == s1, w1, 0.0)
            top = w.astype(BF)
            whi[:, i * SC : (i + 1) * SC] = top
            wlo[:, i * SC : (i + 1) * SC] = (w - top.astype(F32)).astype(BF)

    def ag_part(blk, d, s, q):
        if s < S:
            return xb.at[blk, pl.ds(q * QS, QS), :]
        return xb.at[blk, pl.ds(q * QS + d * (QS // 2), QS // 2), :]

    def ag(d, s, q, incoming):
        ref = ag_part((y + Y - sign[d] * (s if incoming else s - 1)) % Y, d, s, q)
        return remote(ref, ref, ag_s, ag_r.at[d, s - 1, q], ring[d])

    def gate_up(blk):
        return dot(xb[blk], wgu[pl.ds(pl.multiple_of(blk * CW, CW), CW), :])

    def near_arrived():
        @pl.when(active)
        def _():
            settle(xn.at[pl.ds(0, RN - CAP), :], a2a_r.at[NF])

        @pl.when(jnp.logical_not(active))
        def _():
            settle(xn, a2a_r.at[NF])

    def finish(both, rows):
        g = both[:, 0 : 2 * FW]
        hid[rows, :] = (g / (1.0 + jnp.exp(-g)) * both[:, 2 * FW :]).astype(BF)

    def columns_of(dest, half):
        return pl.ds(pl.multiple_of(dest * CW + half * CH, CH), CH)

    def mixer_partial(dest):
        cols = pl.ds(pl.multiple_of(dest * CW, CW), CW)
        mine = gsc[pl.ds(pl.multiple_of(k * MH, MH), MH), :]
        return dot(mine[:, 0:HC], wmo[0:HC, cols]) + dot(gpart[:, 0:HC], wmo[HC:, cols])

    def mx(d, s):
        rows = slice(d * MQ, (d + 1) * MQ) if s == 1 else slice(0, MH)
        rows = pl.ds(rows.start, rows.stop - rows.start)
        return remote(
            msbuf.at[d, s - 1, rows, :], mrbuf.at[d, s - 1, rows, :], mx_s, mx_r.at[d, s - 1], ring[d]
        )

    def mx_step(s):
        for d in range(2):
            b = mixer_partial((y + Y + sign[d] * (S + 1 - s)) % Y)
            msbuf[d, s - 1] = b.astype(BF)
            late = slice(d * MQ, (d + 1) * MQ)
            if s > 1:
                mx(d, s - 1).wait_recv()
                rows = late if s == 2 else slice(0, MH)
                msbuf[d, s - 1, rows, :] = (b[rows] + mrbuf[d, s - 2, rows, :].astype(F32)).astype(BF)
            mx(d, s).start()

    def mx_total():
        b = mixer_partial(y)
        for d in range(2):
            mx(d, S).wait_recv()
            b = b + mrbuf[d, S - 1].astype(F32)
        mout[pl.ds(pl.multiple_of(k * MH, MH), MH), cols_y] = b.astype(BF)

    mixer_steps = [functools.partial(mx_step, s) for s in range(1, S + 1)] + [mx_total]

    def mixer_on():
        if mixer_steps:
            mixer_steps.pop(0)()

    def partial(q, dest):
        return dot(hid[q % 2 * RH : (q % 2 + 1) * RH, :], wd[:, columns_of(dest, q // 2)])

    def slot(d, s, q):
        return d * 2 + q // 2 if s == 1 else 4 + ((s - 2) * 2 + d) * 4 + q

    def rs(d, s, q):
        i = slot(d, s, q)
        return remote(sbuf.at[i], rbuf.at[i], rs_s, rs_r.at[i], ring[d])

    def rs_step(d, s, q):
        a = partial(q, (y + Y + sign[d] * (S + 1 - s)) % Y)
        if s > 2 or (s == 2 and q % 2 == d):
            rs(d, s - 1, q).wait_recv()
            a = a + rbuf[slot(d, s - 1, q)].astype(F32)
        sbuf[slot(d, s, q)] = a.astype(BF)
        rs(d, s, q).start()

    for s in range(1, S + 2):
        for q in range(NF):
            if s == 1:
                settle(xb.at[y, pl.ds(q * QS, QS), :], a2a_r.at[q])
            for d in range(2):
                if s > 1:
                    ag(d, s - 1, q, True).wait_recv()
                if s <= S:
                    ag(d, s, q, False).start()
            if s == 2 and q == 0:
                for i in (5, 6):
                    loads[i].wait()
                weights[0].wait_recv()
                weights[1].wait_recv()
                acc[...] = gate_up(y)
            if s > 2 and q == 0:
                acc[...] += gate_up((y + Y - s + 2) % Y)
            if s > 2 and q == NF // 2:
                acc[...] += gate_up((y + s - 2) % Y)
        if s == S + 1:
            finish(acc[...] + gate_up((y + S) % Y), slice(0, RF))
        if s == S:
            loads[8].wait()
            weights[3].wait_recv()
            send_g.wait_recv()
            near_arrived()
            finish(dot(xn[...], wgu[...]), slice(RF, R))
            mixer_on()
            loads[7].wait()
            weights[2].wait_recv()
        if s == S - 1:
            send_halo.wait_recv()
            ext[0:16, :] = jnp.where(c > 0, halo[...].astype(F32), 0.0)
            ext[16:, :] = ci[...].astype(F32)
            conv = taps[0:1, :] * ext[14 : 14 + M, 0:HC]
            conv = conv + taps[1:2, :] * ext[15 : 15 + M, 0:HC]
            conv = conv + taps[2:3, :] * ext[16 : 16 + M, 0:HC]
            gsc[...] = jnp.zeros(gsc.shape, BF)
            gsc[:, 0:HC] = (go[:, 0:HC] * conv).astype(BF)
            send_g = remote(
                gsc.at[pl.ds(pl.multiple_of((1 - k) * MH, MH), MH), :], gpart, g_s, g_r, partner
            )
            send_g.start()

    turns = [(0, 1), (1, 2), (2, 1), (3, 2)]
    for s in range(2, S):
        turns += [(0, s), (1, s + 1), (2, s), (3, s + 1)]
    turns += [(0, S), (2, S)]
    for n, (q, s) in enumerate(turns):
        for d in range(2):
            rs_step(d, s, q ^ d)
        if n % 4 == 1:
            mixer_on()
    while mixer_steps:
        mixer_on()

    def mixer_piece(core, rel, h):
        cols = pl.ds(pl.multiple_of(((y + Y + rel) % Y) * CW, CW), CW)
        if h is None:
            return mout.at[pl.ds(pl.multiple_of(core * MH, MH), MH), cols]
        return mout.at[pl.ds(pl.multiple_of(core * MH + h * MQ, MQ), MQ), cols]

    def mg(d, s, incoming):
        ref = mixer_piece(k, -sign[d] * (s if incoming else s - 1), None if s < S else d)
        return remote(ref, ref, mg_s, mg_r.at[d, s - 1], ring[d])

    mixer_pieces = [(0, None)]
    for s in range(1, S):
        mixer_pieces += [(-s, None), (s, None)]
    mixer_pieces += [(S, 0), (S, 1)]

    def md(i, core):
        ref = mixer_piece(core, *mixer_pieces[i])
        return remote(ref, ref, md_s, md_r, partner)

    def mg_on(s):
        for d in range(2):
            if s > 1:
                mg(d, s - 1, True).wait_recv()
            if s <= S:
                mg(d, s, False).start()
            if s > 1:
                md(1 + (s - 2) * 2 + d, k).start()

    mg_on(1)
    md(0, k).start()

    def target(i):
        zc = (z + Z + order_off[i // (X // 2)]) % Z
        return zc * X + i % (X // 2) * 2 + k

    def giving(i, half):
        return remote(
            fin.at[half, pl.ds(i * CAP, CAP), :],
            ret.at[half, cap_rows(c), :],
            ret_s,
            ret_r.at[half],
            (target(i), t),
        )

    def distance(i):
        g = order_off[i // (X // 2)] % Z
        return min(g, Z - g)

    own = [i for i in range(E // 2) if order_off[i // (X // 2)] == 0]

    def unless_own(i, act):
        if i in own:
            pl.when(target(i) != c)(act)
        else:
            act()

    def total(q):
        a = partial(q, y)
        for d in range(2):
            rs(d, S, q).wait_recv()
            a = a + rbuf[slot(d, S, q)].astype(F32)
        half, rows = q // 2, q % 2
        fin[half, rows * RH : (rows + 1) * RH, :] = a.astype(BF)
        for i in sorted(range(rows * E // 4, (rows + 1) * E // 4), key=distance, reverse=True):
            unless_own(i, lambda: giving(i, half).start())

    total(0)
    total(1)

    total(2)
    total(3)
    mg_on(2)

    @pl.when(active)
    def _():
        for half in range(2):
            ret[half, cap_rows(c), :] = fin[half, cap_rows(own[0] + x // 2), :]

    def routed_piece(rel, h):
        return rout.at[pl.ds(h % 2 * (T // 2), T // 2), columns_of((y + Y + rel) % Y, h // 2)]

    def pieces(j):
        return [(d, h) for h in range(4) for d in range(2) if j < S or h % 2 == d]

    def rg(d, j, h, incoming):
        if incoming:
            ref = routed_piece(-sign[d] * j, h)
        else:
            ref = routed_piece(0 if j <= 2 else -sign[d] * 2, h)
        dev = (c, ((y + Y + sign[d] * (j if j <= 2 else j - 2)) % Y) * 2 + k)
        return remote(ref, ref, rg_s, ag_r.at[d, j - 1, h], dev)

    def rd(d, j, h):
        ref = routed_piece(-sign[d] * j, h)
        return remote(ref, ref, rd_s, rd_r, partner)

    @pl.when(active)
    def _():
        for half in range(2):

            settle(ret.at[half, pl.ds(0, NS - CAP), :], ret_r.at[half])
            for h in range(2):
                rows = slice(h * (T // 2), (h + 1) * (T // 2))
                weighted = dot(whi[rows, :], ret[half]) + dot(wlo[rows, :], ret[half])
                rout[rows, columns_of(y, half)] = weighted.astype(BF)
                for d, i in pieces(2):
                    if i == 2 * half + h:
                        rg(d, 2, i, False).start()
                rd(0, 0, 2 * half + h).start()
            for d, i in pieces(1):
                if i // 2 == half:
                    rg(d, 1, i, False).start()
        for half in range(2):
            mg_on(3 + half)
            for d, h in pieces(2):
                if h // 2 == half:
                    rg(d, 2, h, True).wait_recv()
                    for j in range(S, 2, -1):
                        if (d, h) in pieces(j):
                            rg(d, j, h, False).start()
                    rd(d, 2, h).start()
        for half in range(2):
            for j in [1] + list(range(3, S + 1)):
                for d, h in pieces(j):
                    if h // 2 == half:
                        rg(d, j, h, True).wait_recv()
                        rd(d, j, h).start()
        for s in range(5, S + 2):
            mg_on(s)

    @pl.when(jnp.logical_not(active))
    def _():
        for s in range(3, S + 2):
            mg_on(s)

    settle(mout.at[pl.ds(0, MH), :], md_s)
    settle(mout.at[pl.ds(0, MH), :], md_r)
    settle(mout.at[pl.ds(0, MH), pl.ds(0, D - CW)], mg_s)
    settle(mout.at[pl.ds(0, MH), pl.ds(0, D - CW)], mx_s)
    settle(xb.at[pl.ds(0, Y - 1)], ag_s)
    settle(sbuf, rs_s)
    for one in weights:
        one.wait_send()
    send_halo.wait_send()
    send_g.wait_send()
    @pl.when(active)
    def _():
        settle(fin.at[:, pl.ds(0, R - CAP), :], ret_s)
        settle(xs, a2a_s.at[0])
        settle(xsn.at[pl.ds(0, NN * PS - CAP), :], a2a_s.at[1])
        settle(rout.at[:, pl.ds(0, D - CW)], rg_s)
        settle(rout, rd_s)

    @pl.when(jnp.logical_not(active))
    def _():
        settle(fin, ret_s)
        settle(rout, rd_r)


def on_device(E, Y, mrows, mgain, win, wgi, wgo, taps, wmo, rrows, rgain, ids, rw, eg, eu, ed):
    M, D = mrows.shape
    T = rrows.shape[0]
    HC = win.shape[1]
    FW = eg.shape[2]
    CW = D // Y
    S = Y // 2
    CAP = 2 * T * ids.shape[1] // E
    X = 4
    NW = 1 if E // X > 3 else 0
    NF = E // X - 2 * NW - 1
    R = E * CAP // 2
    RN = (2 * NW + 1) * (X // 2) * CAP
    VM = pl.BlockSpec(memory_space=pltpu.VMEM)
    HB = pl.BlockSpec(memory_space=pl.ANY)
    DS = pltpu.SemaphoreType.DMA
    return pl.pallas_call(
        functools.partial(kernel, E, Y, X, NW, CAP),
        out_shape=(pltpu.VMEM((M, D), BF), pltpu.VMEM((T, D), BF)),
        in_specs=[HB] * 14,
        out_specs=(VM, VM),
        scratch_shapes=[
            pltpu.VMEM((1, D), F32),
            pltpu.VMEM(taps.shape, F32),
            pltpu.VMEM((1, D), F32),
            pltpu.VMEM((2, T), jnp.int32),
            pltpu.VMEM((2, T), F32),
            pltpu.VMEM((M, D), BF),
            pltpu.VMEM((M, D), BF),
            pltpu.VMEM((HC, D), BF),
            pltpu.VMEM((HC, D), BF),
            pltpu.VMEM((HC, D), BF),
            pltpu.VMEM((2 * HC, D), BF),
            pltpu.VMEM((T, D), BF),
            pltpu.VMEM((T, CW), BF),
            pltpu.VMEM((T, D), BF),
            pltpu.VMEM((T, 128), F32),
            pltpu.VMEM((D, 4 * FW), BF),
            pltpu.VMEM((2 * FW, D), BF),
            pltpu.VMEM((8, T), F32),
            pltpu.VMEM(((R - RN) * 2, CW), BF),
            pltpu.VMEM((2 * RN, D), BF),
            pltpu.VMEM((Y, R - RN, CW), BF),
            pltpu.VMEM((RN, D), BF),
            pltpu.VMEM((R - RN, 4 * FW), F32),
            pltpu.VMEM((R, 2 * FW), BF),
            pltpu.VMEM((8 * S - 4, R // 2, CW // 2), BF),
            pltpu.VMEM((8 * S - 4, R // 2, CW // 2), BF),
            pltpu.VMEM((2, S, M // 2, CW), BF),
            pltpu.VMEM((2, S, M // 2, CW), BF),
            pltpu.VMEM((2, R, CW // 2), BF),
            pltpu.VMEM((2, E * CAP, CW // 2), BF),
            pltpu.VMEM((T, E * CAP), BF),
            pltpu.VMEM((T, E * CAP), BF),
            pltpu.VMEM((M, 128), BF),
            pltpu.VMEM((16, 128), BF),
            pltpu.VMEM((M + 16, 128), F32),
            pltpu.VMEM((M, 128), F32),
            pltpu.VMEM((M, 128), BF),
            pltpu.VMEM((M // 2, 128), BF),
            DS((14,)),
            DS((4,)),
            DS((4,)),
            DS((2,)),
            DS((NF + 1,)),
            DS,
            DS,
            DS,
            DS,
            DS,
            DS((2, S, max(NF, 4))),
            DS,
            DS((8 * S - 4,)),
            DS,
            DS((2, S)),
            DS,
            DS((2,)),
            DS,
            DS((2, S)),
            DS,
            DS,
            DS,
            DS,
            DS,
        ],
        compiler_params=pltpu.CompilerParams(collective_id=0, has_side_effects=True),
    )(
        mrows,
        mgain.reshape(1, D),
        win.T,
        wgi.T,
        wgo.T,
        taps,
        wmo,
        rrows,
        rgain.reshape(1, D),
        ids.T,
        rw.T,
        eg,
        eu,
        ed,
    )


def solution(mesh):
    E = mesh.shape["ep"]
    Y = mesh.shape["tp"] // 2
    return jax.shard_map(
        functools.partial(on_device, E, Y),
        mesh=mesh,
        in_specs=(
            P("ep", None),
            P(),
            P(None, "tp"),
            P(None, "tp"),
            P(None, "tp"),
            P(None, "tp"),
            P("tp", None),
            P("ep", None),
            P(),
            P("ep", None),
            P("ep", None),
            P("ep", None, "tp"),
            P("ep", None, "tp"),
            P("ep", "tp", None),
        ),
        out_specs=(P("ep", None), P("ep", None)),
        check_vma=False,
    )
```

```python
import functools

import jax
import jax.numpy as jnp
from jax import lax
from jax.experimental import pallas as pl
from jax.experimental.pallas import tpu as pltpu
from jax.sharding import PartitionSpec as P

MESH = pl.DeviceIdType.MESH
BF = jnp.bfloat16
F32 = jnp.float32
EPS = 1e-06


def dot(a, b):
    return jnp.dot(a, b, preferred_element_type=F32)


def plan(Z):
    every = [(g, u) for g in sorted(range(Z), key=lambda g: min(g, Z - g)) for u in range(2)]
    reach = 1 if Z > 4 else 0
    near = [b for b in every if min(b[0], Z - b[0]) <= reach]
    if reach:
        near += [(2, 0), (Z - 2, 0)]
    return near, sorted([b for b in every if b not in near], key=lambda b: min(b[0], Z - b[0]))


def dot_t(a, b):
    return lax.dot_general(a, b, (((1,), (1,)), ((), ())), preferred_element_type=F32)


def kernel(
    E,
    Y,
    X,
    CAP,
    mrows_hbm,
    mgain_hbm,
    win_hbm,
    wgi_hbm,
    wgo_hbm,
    taps_hbm,
    wmo_hbm,
    rrows_hbm,
    rgain_hbm,
    ids_hbm,
    rw_hbm,
    eg_hbm,
    eu_hbm,
    ed_hbm,
    mout,
    rout,
    mgain,
    taps,
    rgain,
    ids_ref,
    rw_ref,
    mrows,
    mn,
    win,
    wgi,
    wgo,
    wmo,
    rrows,
    nrm,
    nfull,
    rscale,
    wgu,
    wd,
    slotrow,
    xs,
    xsn,
    xb,
    xn,
    acc,
    hid,
    sbuf,
    rbuf,
    msbuf,
    mrbuf,
    fin,
    ret,
    whi,
    wlo,
    ci,
    halo,
    ext,
    go,
    gsc,
    gpart,
    l_sem,
    wt_s,
    wt_r,
    a2a_s,
    a2a_r,
    halo_s,
    halo_r,
    g_s,
    g_r,
    ag_s,
    ag_r,
    rs_s,
    rs_r,
    mx_s,
    mx_r,
    ret_s,
    ret_r,
    mg_s,
    mg_r,
    md_s,
    md_r,
    rg_s,
    rd_s,
    rd_r,
):
    S = Y // 2
    c = lax.axis_index("ep")
    t = lax.axis_index("tp")
    y = t // 2
    k = t % 2
    z = c // X
    x = c % X
    active = k == c % 2
    M, D = mn.shape
    T = nrm.shape[0]
    CW = D // Y
    NS = E * CAP
    R = NS // 2
    Z = E // X
    near_blocks, far_blocks = plan(Z)
    blocks = near_blocks + far_blocks
    NF = len(far_blocks) // 2
    RN = len(near_blocks) * CAP
    RF = len(far_blocks) * CAP
    QS = 2 * CAP
    RH = R // 2
    CH = CW // 2
    MH = M // 2
    MQ = MH // 2
    HC = win.shape[0]
    EP = -(-E // 16) * 16
    partner = (c, y * 2 + 1 - k)
    ring = [(c, ((y + 1) % Y) * 2 + k), (c, ((y + Y - 1) % Y) * 2 + k)]
    sign = [1, -1]

    def remote(src, dst, ss, rs, dev):
        return pltpu.make_async_remote_copy(
            src_ref=src, dst_ref=dst, send_sem=ss, recv_sem=rs, device_id=dev, device_id_type=MESH
        )

    def settle(ref, sem):
        pltpu.make_async_copy(ref, ref, sem).wait()

    FW = eg_hbm.shape[2]
    loads = [
        pltpu.make_async_copy(rrows_hbm, rrows, l_sem.at[0]),
        pltpu.make_async_copy(mrows_hbm, mrows, l_sem.at[1]),
        pltpu.make_async_copy(win_hbm, win, l_sem.at[2]),
        pltpu.make_async_copy(wgi_hbm, wgi, l_sem.at[3]),
        pltpu.make_async_copy(wgo_hbm, wgo, l_sem.at[4]),
        pltpu.make_async_copy(eg_hbm.at[0], wgu.at[:, pl.ds(0, FW)], l_sem.at[5]),
        pltpu.make_async_copy(eu_hbm.at[0], wgu.at[:, pl.ds(2 * FW, FW)], l_sem.at[6]),
        pltpu.make_async_copy(ed_hbm.at[0], wd.at[pl.ds(0, FW), :], l_sem.at[7]),
        pltpu.make_async_copy(wmo_hbm, wmo.at[pl.ds(0, HC), :], l_sem.at[8]),
        pltpu.make_async_copy(ids_hbm, ids_ref, l_sem.at[9]),
        pltpu.make_async_copy(rw_hbm, rw_ref, l_sem.at[10]),
        pltpu.make_async_copy(rgain_hbm, rgain, l_sem.at[11]),
        pltpu.make_async_copy(mgain_hbm, mgain, l_sem.at[12]),
        pltpu.make_async_copy(taps_hbm, taps, l_sem.at[13]),
    ]
    for i in (9, 0, 11):
        loads[i].start()

    barrier = pltpu.get_barrier_semaphore()

    for g in sorted(range(Z), key=lambda g: -min(g, Z - g)):

        def greet(i, carry):
            there = (z + g) % Z * X + (x + i) % X
            pl.semaphore_signal(barrier, inc=1, device_id=(there, t), device_id_type=MESH)
            return carry

        lax.fori_loop(0 if g else 1, X, greet, 0)
    for dev in (partner, ring[0], ring[1]):
        pl.semaphore_signal(barrier, inc=1, device_id=dev, device_id_type=MESH)

    for i in (1, 12, 2, 3, 4, 10, 13, 5, 6, 7, 8):
        loads[i].start()

    def slot_numbers():
        ids = ids_ref[...]
        expert = lax.broadcasted_iota(jnp.int32, (EP, T), 0)
        hit0 = expert == ids[0:1, :]
        hit1 = expert == ids[1:2, :]
        named = jnp.where(hit0 | hit1, 1.0, 0.0).astype(BF)
        r = lax.broadcasted_iota(jnp.int32, (T, T), 0)
        q = lax.broadcasted_iota(jnp.int32, (T, T), 1)
        upper = jnp.where(r < q, 1.0, 0.0).astype(BF)
        before = dot(named, upper)
        row0 = ids[0:1, :].astype(F32) * CAP + jnp.sum(
            jnp.where(hit0, before, 0.0), axis=0, keepdims=True
        )
        row1 = ids[1:2, :].astype(F32) * CAP + jnp.sum(
            jnp.where(hit1, before, 0.0), axis=0, keepdims=True
        )
        return row0, row1

    def slot_columns():
        r = lax.broadcasted_iota(jnp.int32, (T, T), 0)
        q = lax.broadcasted_iota(jnp.int32, (T, T), 1)
        diag = r == q
        rows = (slotrow[0:1, :], slotrow[1:2, :], rw_ref[0:1, :], rw_ref[1:2, :])
        return [jnp.sum(jnp.where(diag, row, 0.0), axis=1, keepdims=True) for row in rows]

    cols_y = pl.ds(pl.multiple_of(y * CW, CW), CW)

    def norm_routed():
        step = 32

        def body(i, carry):
            rows = pl.ds(pl.multiple_of(i * step, step), step)
            v = rrows[rows, :].astype(F32)
            scale = lax.rsqrt(jnp.mean(v * v, axis=-1, keepdims=True) + EPS)
            rscale[rows, :] = jnp.broadcast_to(scale, (step, 128))
            part = rrows[rows, cols_y].astype(F32)
            nrm[rows, :] = (part * scale * rgain[:, cols_y]).astype(BF)
            return carry

        lax.fori_loop(0, T // step, body, 0)

    loads[9].wait()

    SC = NS // 4

    def cap_rows(i):
        return pl.ds(pl.multiple_of(i * CAP, CAP), CAP)

    def there(g, u, i):
        return (z + Z - g) % Z * X + (x // 2 ^ u) * 2 + i

    def far(b, i):
        return remote(
            xs.at[cap_rows(2 * b + i), :],
            xb.at[y, pl.ds(b * CAP, CAP), :],
            a2a_s.at[0],
            a2a_r.at[b // 2],
            (there(*far_blocks[b], i), t),
        )

    def near(b, i):
        return remote(
            xsn.at[cap_rows(2 * b + i), :],
            xn.at[pl.ds(b * CAP, CAP), :],
            a2a_s.at[1],
            a2a_r.at[NF],
            (there(*near_blocks[b], i), t),
        )

    OWN = near_blocks.index((0, 0))

    def pick(group):
        row0 = slotrow[0:1, :].astype(jnp.int32)
        row1 = slotrow[1:2, :].astype(jnp.int32)
        parts = []
        for g, u in group:
            number = lax.broadcasted_iota(jnp.int32, (2 * CAP, T), 0) + there(g, u, 0) * CAP
            parts.append(jnp.where((number == row0) | (number == row1), 1.0, 0.0).astype(BF))
        return jnp.concatenate(parts, axis=0)

    @pl.when(active)
    def _():
        row0, row1 = slot_numbers()
        loads[0].wait()
        loads[11].wait()
        norm_routed()
        slotrow[0:1, :] = row0
        slotrow[1:2, :] = row1

        xs[...] = dot(pick(far_blocks), nrm[...]).astype(BF)

    @pl.when(jnp.logical_not(active))
    def _():
        for i in (0, 10, 11):
            loads[i].wait()

    pl.semaphore_wait(barrier, E + 2)

    @pl.when(active)
    def _():
        for b in range(len(far_blocks)):
            for i in range(2):
                far(b, i).start()

    weights = [
        remote(eg_hbm.at[0], wgu.at[:, pl.ds(FW, FW)], wt_s.at[0], wt_r.at[0], partner),
        remote(eu_hbm.at[0], wgu.at[:, pl.ds(3 * FW, FW)], wt_s.at[1], wt_r.at[1], partner),
        remote(ed_hbm.at[0], wd.at[pl.ds(FW, FW), :], wt_s.at[2], wt_r.at[2], partner),
        remote(wmo_hbm, wmo.at[pl.ds(HC, HC), :], wt_s.at[3], wt_r.at[3], partner),
    ]
    for one in weights:
        one.start()

    for i in (1, 2, 3, 4, 12, 13):
        loads[i].wait()

    def norm_mixer(i, carry):
        rows = pl.ds(pl.multiple_of(i * 16, 16), 16)
        v = mrows[rows, :].astype(F32)
        scale = lax.rsqrt(jnp.mean(v * v, axis=-1, keepdims=True) + EPS)
        mn[rows, :] = (v * scale * mgain[...]).astype(BF)
        return carry

    lax.fori_loop(0, M // 16, norm_mixer, 0)
    normed = mn[...]
    inner = dot_t(normed, win[...])
    gate_in = dot_t(normed, wgi[...])
    go[:, 0:HC] = dot_t(normed, wgo[...])
    ci[...] = jnp.zeros(ci.shape, BF)
    ci[:, 0:HC] = (gate_in * inner).astype(BF)
    send_halo = remote(ci.at[pl.ds(M - 16, 16), :], halo, halo_s, halo_r, ((c + 1) % E, t))
    send_halo.start()

    @pl.when(active)
    def _():
        def norm_full(i, carry):
            rows = pl.ds(pl.multiple_of(i * 16, 16), 16)
            v = rrows[rows, :].astype(F32)
            nfull[rows, :] = (v * rscale[rows, 0:1] * rgain[...]).astype(BF)
            return carry

        lax.fori_loop(0, T // 16, norm_full, 0)

        for first in range(0, len(near_blocks), 4):
            group = near_blocks[first : first + 4]
            rows = slice(2 * first * CAP, 2 * (first + len(group)) * CAP)
            xsn[rows, :] = dot(pick(group), nfull[...]).astype(BF)
        for b in range(len(near_blocks) - 1, -1, -1):
            for i in range(2):
                if b == OWN:
                    pl.when(x % 2 != i)(lambda: near(b, i).start())
                else:
                    near(b, i).start()
        xn[OWN * CAP : (OWN + 1) * CAP, :] = xsn[cap_rows(2 * OWN + x % 2), :]

        loads[10].wait()
        s0, s1, w0, w1 = slot_columns()
        s0 = s0.astype(jnp.int32)
        s1 = s1.astype(jnp.int32)
        for i in range(4):
            number = lax.broadcasted_iota(jnp.int32, (T, SC), 1) + i * SC
            w = jnp.where(number == s0, w0, 0.0) + jnp.where(number == s1, w1, 0.0)
            top = w.astype(BF)
            whi[:, i * SC : (i + 1) * SC] = top
            wlo[:, i * SC : (i + 1) * SC] = (w - top.astype(F32)).astype(BF)

    def ag_part(blk, d, s, q):
        if s < S:
            return xb.at[blk, pl.ds(q * QS, QS), :]
        return xb.at[blk, pl.ds(q * QS + d * (QS // 2), QS // 2), :]

    def ag(d, s, q, incoming):
        ref = ag_part((y + Y - sign[d] * (s if incoming else s - 1)) % Y, d, s, q)
        return remote(ref, ref, ag_s, ag_r.at[d, s - 1, q], ring[d])

    def gate_up(blk, rows=slice(None)):
        return dot(xb[blk, rows, :], wgu[pl.ds(pl.multiple_of(blk * CW, CW), CW), :])

    def near_arrived():
        @pl.when(active)
        def _():
            settle(xn.at[pl.ds(0, RN - CAP), :], a2a_r.at[NF])

        @pl.when(jnp.logical_not(active))
        def _():
            settle(xn, a2a_r.at[NF])

    def finish(both, rows):
        g = both[:, 0 : 2 * FW]
        hid[rows, :] = (g / (1.0 + jnp.exp(-g)) * both[:, 2 * FW :]).astype(BF)

    def columns_of(dest, half):
        return pl.ds(pl.multiple_of(dest * CW + half * CH, CH), CH)

    def mixer_partial(dest):
        cols = pl.ds(pl.multiple_of(dest * CW, CW), CW)
        mine = gsc[pl.ds(pl.multiple_of(k * MH, MH), MH), :]
        return dot(mine[:, 0:HC], wmo[0:HC, cols]) + dot(gpart[:, 0:HC], wmo[HC:, cols])

    def mx(d, s):
        rows = slice(d * MQ, (d + 1) * MQ) if s == 1 else slice(0, MH)
        rows = pl.ds(rows.start, rows.stop - rows.start)
        return remote(
            msbuf.at[d, s - 1, rows, :], mrbuf.at[d, s - 1, rows, :], mx_s, mx_r.at[d, s - 1], ring[d]
        )

    def mx_step(s):
        for d in range(2):
            b = mixer_partial((y + Y + sign[d] * (S + 1 - s)) % Y)
            msbuf[d, s - 1] = b.astype(BF)
            late = slice(d * MQ, (d + 1) * MQ)
            if s > 1:
                mx(d, s - 1).wait_recv()
                rows = late if s == 2 else slice(0, MH)
                msbuf[d, s - 1, rows, :] = (b[rows] + mrbuf[d, s - 2, rows, :].astype(F32)).astype(BF)
            mx(d, s).start()

    def mx_total():
        b = mixer_partial(y)
        for d in range(2):
            mx(d, S).wait_recv()
            b = b + mrbuf[d, S - 1].astype(F32)
        mout[pl.ds(pl.multiple_of(k * MH, MH), MH), cols_y] = b.astype(BF)

    mixer_steps = [functools.partial(mx_step, s) for s in range(1, S + 1)] + [mx_total]

    def mixer_on():
        if mixer_steps:
            mixer_steps.pop(0)()

    def partial(q, dest):
        return dot(hid[q % 2 * RH : (q % 2 + 1) * RH, :], wd[:, columns_of(dest, q // 2)])

    def slot(d, s, q):
        return d * 2 + q // 2 if s == 1 else 4 + ((s - 2) * 2 + d) * 4 + q

    def rs(d, s, q):
        i = slot(d, s, q)
        return remote(sbuf.at[i], rbuf.at[i], rs_s, rs_r.at[i], ring[d])

    def rs_step(d, s, q):
        a = partial(q, (y + Y + sign[d] * (S + 1 - s)) % Y)
        if s > 2 or (s == 2 and q % 2 == d):
            rs(d, s - 1, q).wait_recv()
            a = a + rbuf[slot(d, s - 1, q)].astype(F32)
        sbuf[slot(d, s, q)] = a.astype(BF)
        rs(d, s, q).start()

    def mixer_rest():
        send_halo.wait_recv()
        ext[0:16, :] = jnp.where(c > 0, halo[...].astype(F32), 0.0)
        ext[16:, :] = ci[...].astype(F32)
        conv = taps[0:1, :] * ext[14 : 14 + M, 0:HC]
        conv = conv + taps[1:2, :] * ext[15 : 15 + M, 0:HC]
        conv = conv + taps[2:3, :] * ext[16 : 16 + M, 0:HC]
        gsc[...] = jnp.zeros(gsc.shape, BF)
        gsc[:, 0:HC] = (go[:, 0:HC] * conv).astype(BF)
        send_g = remote(
            gsc.at[pl.ds(pl.multiple_of((1 - k) * MH, MH), MH), :], gpart, g_s, g_r, partner
        )
        send_g.start()
        return send_g

    def own_products():
        for i in (5, 6):
            loads[i].wait()
        weights[0].wait_recv()
        weights[1].wait_recv()
        acc[...] = gate_up(y)

    def products(rel):
        acc[...] += gate_up((y + Y + rel) % Y)

    hop = 2.75
    steps = [(s, q) for s in range(1, S + 1) for q in range(NF)]
    steps.sort(key=lambda one: (one[1] + hop * (one[0] - 1), -one[0]))
    waiting = []
    for s, q in steps:
        if s == 1:
            settle(xb.at[y, pl.ds(q * QS, QS), :], a2a_r.at[q])
        else:
            pass
        for d in range(2):
            if s > 1:
                ag(d, s - 1, q, True).wait_recv()
            ag(d, s, q, False).start()
        if q == NF - 1:
            waiting += [own_products] if s == 1 else [
                functools.partial(products, s - 1),
                functools.partial(products, 1 - s),
            ]
        if waiting:
            waiting.pop(0)()
        if (s, q) == (2, 0):
            send_g = mixer_rest()
            loads[8].wait()
        if (s, q) == (2, min(1, NF - 1)):
            weights[3].wait_recv()
            send_g.wait_recv()
        if (s, q) in ((2, min(1, NF - 1)), (3, 2), (4, 3)):
            mixer_on()
    for one in waiting:
        one()
    near_arrived()
    finish(dot(xn[...], wgu[...]), slice(0, RN))
    early = [(0, 1, 0), (1, 2, 0), (0, 1, 2), (1, 2, 2)]
    loads[7].wait()
    weights[2].wait_recv()
    for one in early:
        rs_step(*one)
    for q in range(NF):
        for d in range(2):
            ag(d, S, q, True).wait_recv()
    finish(acc[...] + gate_up((y + S) % Y), slice(RN, R))

    turns = [(0, 1), (1, 2), (2, 1), (3, 2)]
    for s in range(2, S):
        turns += [(0, s), (1, s + 1), (2, s), (3, s + 1)]
    turns += [(0, S), (2, S)]
    for n, (q, s) in enumerate(turns):
        for d in range(2):
            if (d, s, q ^ d) not in early:
                rs_step(d, s, q ^ d)
        if n in (1, 6):
            mixer_on()
    while mixer_steps:
        mixer_on()

    def mixer_piece(core, rel, h):
        cols = pl.ds(pl.multiple_of(((y + Y + rel) % Y) * CW, CW), CW)
        if h is None:
            return mout.at[pl.ds(pl.multiple_of(core * MH, MH), MH), cols]
        return mout.at[pl.ds(pl.multiple_of(core * MH + h * MQ, MQ), MQ), cols]

    def mg(d, j, incoming):
        h = None if j < S else d
        if incoming:
            ref = mixer_piece(k, -sign[d] * j, h)
        else:
            ref = mixer_piece(k, 0 if j <= 2 else -sign[d] * 2, h)
        dev = (c, ((y + Y + sign[d] * (j if j <= 2 else j - 2)) % Y) * 2 + k)
        return remote(ref, ref, mg_s, mg_r.at[d, j - 1], dev)

    def md(d, j):
        ref = mixer_piece(k, -sign[d] * j, None if j < S else d)
        return remote(ref, ref, md_s, md_r, partner)

    def mixer_arrived(j):
        for d in range(2):
            mg(d, j, True).wait_recv()
            if j == 2:
                for far_j in range(S, 2, -1):
                    mg(d, far_j, False).start()
            md(d, j).start()

    def target(i):
        g, u = blocks[i]
        return (z + g) % Z * X + (x // 2 ^ u) * 2 + k

    def giving(i, half):
        return remote(
            fin.at[half, pl.ds(i * CAP, CAP), :],
            ret.at[half, cap_rows(c), :],
            ret_s,
            ret_r.at[half],
            (target(i), t),
        )

    def distance(i):
        return min(blocks[i][0], Z - blocks[i][0])

    def unless_own(i, act):
        if i == OWN:
            pl.when(target(i) != c)(act)
        else:
            act()

    def total(q):
        a = partial(q, y)
        for d in range(2):
            rs(d, S, q).wait_recv()
            a = a + rbuf[slot(d, S, q)].astype(F32)
        half, rows = q // 2, q % 2
        fin[half, rows * RH : (rows + 1) * RH, :] = a.astype(BF)
        for i in sorted(range(rows * E // 4, (rows + 1) * E // 4), key=distance, reverse=True):
            unless_own(i, lambda: giving(i, half).start())

    total(0)
    total(1)

    total(2)
    total(3)
    for j in (2, 1):
        for d in range(2):
            mg(d, j, False).start()
    remote(mixer_piece(k, 0, None), mixer_piece(k, 0, None), md_s, md_r, partner).start()
    mixer_arrived(2)

    @pl.when(active)
    def _():
        for half in range(2):
            ret[half, cap_rows(c), :] = fin[half, OWN * CAP : (OWN + 1) * CAP, :]

    def routed_piece(rel, h):
        return rout.at[pl.ds(h % 2 * (T // 2), T // 2), columns_of((y + Y + rel) % Y, h // 2)]

    def pieces(j):
        return [(d, h) for h in range(4) for d in range(2) if j < S or h % 2 == d]

    def rg(d, j, h, incoming):
        if incoming:
            ref = routed_piece(-sign[d] * j, h)
        else:
            ref = routed_piece(0 if j <= 2 else -sign[d] * 2, h)
        dev = (c, ((y + Y + sign[d] * (j if j <= 2 else j - 2)) % Y) * 2 + k)
        return remote(ref, ref, rg_s, ag_r.at[d, j - 1, h], dev)

    def rd(d, j, h):
        ref = routed_piece(-sign[d] * j, h)
        return remote(ref, ref, rd_s, rd_r, partner)

    @pl.when(active)
    def _():
        for half in range(2):

            settle(ret.at[half, pl.ds(0, NS - CAP), :], ret_r.at[half])
            for h in range(2):
                rows = slice(h * (T // 2), (h + 1) * (T // 2))
                weighted = dot(whi[rows, :], ret[half]) + dot(wlo[rows, :], ret[half])
                rout[rows, columns_of(y, half)] = weighted.astype(BF)
                for d, i in pieces(2):
                    if i == 2 * half + h:
                        rg(d, 2, i, False).start()
                rd(0, 0, 2 * half + h).start()
            for d, i in pieces(1):
                if i // 2 == half:
                    rg(d, 1, i, False).start()
        for half in range(2):
            for d, h in pieces(2):
                if h // 2 == half:
                    rg(d, 2, h, True).wait_recv()
                    for j in range(S, 2, -1):
                        if (d, h) in pieces(j):
                            rg(d, j, h, False).start()
                    rd(d, 2, h).start()
        for j in [1] + list(range(3, S + 1)):
            mixer_arrived(j)
        for half in range(2):
            for j in [1] + list(range(3, S + 1)):
                for d, h in pieces(j):
                    if h // 2 == half:
                        rg(d, j, h, True).wait_recv()
                        rd(d, j, h).start()

    @pl.when(jnp.logical_not(active))
    def _():
        for j in [1] + list(range(3, S + 1)):
            mixer_arrived(j)

    settle(mout.at[pl.ds(0, MH), :], md_s)
    settle(mout.at[pl.ds(0, MH), :], md_r)
    settle(mout.at[pl.ds(0, MH), pl.ds(0, D - CW)], mg_s)
    settle(mout.at[pl.ds(0, MH), pl.ds(0, D - CW)], mx_s)
    settle(xb.at[pl.ds(0, Y - 1)], ag_s)
    settle(sbuf, rs_s)
    for one in weights:
        one.wait_send()
    send_halo.wait_send()
    send_g.wait_send()
    @pl.when(active)
    def _():
        settle(fin.at[:, pl.ds(0, R - CAP), :], ret_s)
        settle(xs, a2a_s.at[0])
        settle(xsn.at[pl.ds(0, 2 * RN - CAP), :], a2a_s.at[1])
        settle(rout.at[:, pl.ds(0, D - CW)], rg_s)
        settle(rout, rd_s)

    @pl.when(jnp.logical_not(active))
    def _():
        settle(fin, ret_s)
        settle(rout, rd_r)


def on_device(E, Y, mrows, mgain, win, wgi, wgo, taps, wmo, rrows, rgain, ids, rw, eg, eu, ed):
    M, D = mrows.shape
    T = rrows.shape[0]
    HC = win.shape[1]
    FW = eg.shape[2]
    CW = D // Y
    S = Y // 2
    CAP = 2 * T * ids.shape[1] // E
    X = 4
    near_blocks, far_blocks = plan(E // X)
    NF = len(far_blocks) // 2
    R = E * CAP // 2
    RN = len(near_blocks) * CAP
    VM = pl.BlockSpec(memory_space=pltpu.VMEM)
    HB = pl.BlockSpec(memory_space=pl.ANY)
    DS = pltpu.SemaphoreType.DMA
    return pl.pallas_call(
        functools.partial(kernel, E, Y, X, CAP),
        out_shape=(pltpu.VMEM((M, D), BF), pltpu.VMEM((T, D), BF)),
        in_specs=[HB] * 14,
        out_specs=(VM, VM),
        scratch_shapes=[
            pltpu.VMEM((1, D), F32),
            pltpu.VMEM(taps.shape, F32),
            pltpu.VMEM((1, D), F32),
            pltpu.VMEM((2, T), jnp.int32),
            pltpu.VMEM((2, T), F32),
            pltpu.VMEM((M, D), BF),
            pltpu.VMEM((M, D), BF),
            pltpu.VMEM((HC, D), BF),
            pltpu.VMEM((HC, D), BF),
            pltpu.VMEM((HC, D), BF),
            pltpu.VMEM((2 * HC, D), BF),
            pltpu.VMEM((T, D), BF),
            pltpu.VMEM((T, CW), BF),
            pltpu.VMEM((T, D), BF),
            pltpu.VMEM((T, 128), F32),
            pltpu.VMEM((D, 4 * FW), BF),
            pltpu.VMEM((2 * FW, D), BF),
            pltpu.VMEM((8, T), F32),
            pltpu.VMEM(((R - RN) * 2, CW), BF),
            pltpu.VMEM((2 * RN, D), BF),
            pltpu.VMEM((Y, R - RN, CW), BF),
            pltpu.VMEM((RN, D), BF),
            pltpu.VMEM((R - RN, 4 * FW), F32),
            pltpu.VMEM((R, 2 * FW), BF),
            pltpu.VMEM((8 * S - 4, R // 2, CW // 2), BF),
            pltpu.VMEM((8 * S - 4, R // 2, CW // 2), BF),
            pltpu.VMEM((2, S, M // 2, CW), BF),
            pltpu.VMEM((2, S, M // 2, CW), BF),
            pltpu.VMEM((2, R, CW // 2), BF),
            pltpu.VMEM((2, E * CAP, CW // 2), BF),
            pltpu.VMEM((T, E * CAP), BF),
            pltpu.VMEM((T, E * CAP), BF),
            pltpu.VMEM((M, 128), BF),
            pltpu.VMEM((16, 128), BF),
            pltpu.VMEM((M + 16, 128), F32),
            pltpu.VMEM((M, 128), F32),
            pltpu.VMEM((M, 128), BF),
            pltpu.VMEM((M // 2, 128), BF),
            DS((14,)),
            DS((4,)),
            DS((4,)),
            DS((2,)),
            DS((NF + 1,)),
            DS,
            DS,
            DS,
            DS,
            DS,
            DS((2, S, max(NF, 4))),
            DS,
            DS((8 * S - 4,)),
            DS,
            DS((2, S)),
            DS,
            DS((2,)),
            DS,
            DS((2, S)),
            DS,
            DS,
            DS,
            DS,
            DS,
        ],
        compiler_params=pltpu.CompilerParams(collective_id=0, has_side_effects=True),
    )(
        mrows,
        mgain.reshape(1, D),
        win.T,
        wgi.T,
        wgo.T,
        taps,
        wmo,
        rrows,
        rgain.reshape(1, D),
        ids.T,
        rw.T,
        eg,
        eu,
        ed,
    )


def solution(mesh):
    E = mesh.shape["ep"]
    Y = mesh.shape["tp"] // 2
    return jax.shard_map(
        functools.partial(on_device, E, Y),
        mesh=mesh,
        in_specs=(
            P("ep", None),
            P(),
            P(None, "tp"),
            P(None, "tp"),
            P(None, "tp"),
            P(None, "tp"),
            P("tp", None),
            P("ep", None),
            P(),
            P("ep", None),
            P("ep", None),
            P("ep", None, "tp"),
            P("ep", None, "tp"),
            P("ep", "tp", None),
        ),
        out_specs=(P("ep", None), P("ep", None)),
        check_vma=False,
    )
```

```python
import functools

import jax
import jax.numpy as jnp
from jax import lax
from jax.experimental import pallas as pl
from jax.experimental.pallas import tpu as pltpu
from jax.sharding import PartitionSpec as P

MESH = pl.DeviceIdType.MESH
BF = jnp.bfloat16
F32 = jnp.float32
EPS = 1e-06


def dot(a, b):
    return jnp.dot(a, b, preferred_element_type=F32)


def plan(Z):
    every = [(g, u) for g in sorted(range(Z), key=lambda g: min(g, Z - g)) for u in range(2)]
    reach = 1 if Z > 4 else 0
    near = [b for b in every if min(b[0], Z - b[0]) <= reach]
    if reach:
        near += [(2, 0), (Z - 2, 0)]
    return near, sorted([b for b in every if b not in near], key=lambda b: min(b[0], Z - b[0]))


def dot_t(a, b):
    return lax.dot_general(a, b, (((1,), (1,)), ((), ())), preferred_element_type=F32)


def kernel(
    E,
    Y,
    X,
    CAP,
    mrows_hbm,
    mgain_hbm,
    win_hbm,
    wgi_hbm,
    wgo_hbm,
    taps_hbm,
    wmo_hbm,
    rrows_hbm,
    rgain_hbm,
    ids_hbm,
    rw_hbm,
    eg_hbm,
    eu_hbm,
    ed_hbm,
    mout,
    rout,
    mgain,
    taps,
    rgain,
    ids_ref,
    rw_ref,
    mrows,
    mn,
    win,
    wgi,
    wgo,
    wmo,
    rrows,
    nrm,
    nfull,
    rscale,
    wgu,
    wd,
    slotrow,
    xs,
    xsn,
    xb,
    xn,
    acc,
    hid,
    sbuf,
    rbuf,
    msbuf,
    mrbuf,
    fin,
    ret,
    whi,
    wlo,
    ci,
    halo,
    ext,
    go,
    gsc,
    gpart,
    l_sem,
    wt_s,
    wt_r,
    a2a_s,
    a2a_r,
    halo_s,
    halo_r,
    g_s,
    g_r,
    ag_s,
    ag_r,
    rs_s,
    rs_r,
    mx_s,
    mx_r,
    ret_s,
    ret_r,
    mg_s,
    mg_r,
    md_s,
    md_r,
    rg_s,
    rd_s,
    rd_r,
):
    S = Y // 2
    c = lax.axis_index("ep")
    t = lax.axis_index("tp")
    y = t // 2
    k = t % 2
    z = c // X
    x = c % X
    active = k == c % 2
    M, D = mn.shape
    T = nrm.shape[0]
    CW = D // Y
    NS = E * CAP
    R = NS // 2
    Z = E // X
    near_blocks, far_blocks = plan(Z)
    blocks = near_blocks + far_blocks
    NF = len(far_blocks) // 2
    RN = len(near_blocks) * CAP
    RF = len(far_blocks) * CAP
    QS = 2 * CAP
    RH = R // 2
    CH = CW // 2
    MH = M // 2
    MQ = MH // 2
    HC = win.shape[0]
    EP = -(-E // 16) * 16
    partner = (c, y * 2 + 1 - k)
    ring = [(c, ((y + 1) % Y) * 2 + k), (c, ((y + Y - 1) % Y) * 2 + k)]
    sign = [1, -1]

    def remote(src, dst, ss, rs, dev):
        return pltpu.make_async_remote_copy(
            src_ref=src, dst_ref=dst, send_sem=ss, recv_sem=rs, device_id=dev, device_id_type=MESH
        )

    def settle(ref, sem):
        pltpu.make_async_copy(ref, ref, sem).wait()

    FW = eg_hbm.shape[2]
    loads = [
        pltpu.make_async_copy(rrows_hbm, rrows, l_sem.at[0]),
        pltpu.make_async_copy(mrows_hbm, mrows, l_sem.at[1]),
        pltpu.make_async_copy(win_hbm, win, l_sem.at[2]),
        pltpu.make_async_copy(wgi_hbm, wgi, l_sem.at[3]),
        pltpu.make_async_copy(wgo_hbm, wgo, l_sem.at[4]),
        pltpu.make_async_copy(eg_hbm.at[0], wgu.at[:, pl.ds(0, FW)], l_sem.at[5]),
        pltpu.make_async_copy(eu_hbm.at[0], wgu.at[:, pl.ds(2 * FW, FW)], l_sem.at[6]),
        pltpu.make_async_copy(ed_hbm.at[0], wd.at[pl.ds(0, FW), :], l_sem.at[7]),
        pltpu.make_async_copy(wmo_hbm, wmo.at[pl.ds(0, HC), :], l_sem.at[8]),
        pltpu.make_async_copy(ids_hbm, ids_ref, l_sem.at[9]),
        pltpu.make_async_copy(rw_hbm, rw_ref, l_sem.at[10]),
        pltpu.make_async_copy(rgain_hbm, rgain, l_sem.at[11]),
        pltpu.make_async_copy(mgain_hbm, mgain, l_sem.at[12]),
        pltpu.make_async_copy(taps_hbm, taps, l_sem.at[13]),
    ]
    for i in (9, 0, 11):
        loads[i].start()

    barrier = pltpu.get_barrier_semaphore()

    for g in sorted(range(Z), key=lambda g: -min(g, Z - g)):

        def greet(i, carry):
            there = (z + g) % Z * X + (x + i) % X
            pl.semaphore_signal(barrier, inc=1, device_id=(there, t), device_id_type=MESH)
            return carry

        lax.fori_loop(0 if g else 1, X, greet, 0)
    for dev in (partner, ring[0], ring[1]):
        pl.semaphore_signal(barrier, inc=1, device_id=dev, device_id_type=MESH)

    for i in (1, 12, 2, 3, 4, 10, 13, 5, 6, 7, 8):
        loads[i].start()

    def slot_numbers():
        ids = ids_ref[...]
        expert = lax.broadcasted_iota(jnp.int32, (EP, T), 0)
        hit0 = expert == ids[0:1, :]
        hit1 = expert == ids[1:2, :]
        named = jnp.where(hit0 | hit1, 1.0, 0.0).astype(BF)
        r = lax.broadcasted_iota(jnp.int32, (T, T), 0)
        q = lax.broadcasted_iota(jnp.int32, (T, T), 1)
        upper = jnp.where(r < q, 1.0, 0.0).astype(BF)
        before = dot(named, upper)
        row0 = ids[0:1, :].astype(F32) * CAP + jnp.sum(
            jnp.where(hit0, before, 0.0), axis=0, keepdims=True
        )
        row1 = ids[1:2, :].astype(F32) * CAP + jnp.sum(
            jnp.where(hit1, before, 0.0), axis=0, keepdims=True
        )
        return row0, row1

    def slot_columns():
        r = lax.broadcasted_iota(jnp.int32, (T, T), 0)
        q = lax.broadcasted_iota(jnp.int32, (T, T), 1)
        diag = r == q
        rows = (slotrow[0:1, :], slotrow[1:2, :], rw_ref[0:1, :], rw_ref[1:2, :])
        return [jnp.sum(jnp.where(diag, row, 0.0), axis=1, keepdims=True) for row in rows]

    cols_y = pl.ds(pl.multiple_of(y * CW, CW), CW)

    def norm_routed():
        step = 32

        def body(i, carry):
            rows = pl.ds(pl.multiple_of(i * step, step), step)
            v = rrows[rows, :].astype(F32)
            scale = lax.rsqrt(jnp.mean(v * v, axis=-1, keepdims=True) + EPS)
            rscale[rows, :] = jnp.broadcast_to(scale, (step, 128))
            part = rrows[rows, cols_y].astype(F32)
            nrm[rows, :] = (part * scale * rgain[:, cols_y]).astype(BF)
            return carry

        lax.fori_loop(0, T // step, body, 0)

    loads[9].wait()

    SC = NS // 4

    def cap_rows(i):
        return pl.ds(pl.multiple_of(i * CAP, CAP), CAP)

    def there(g, u, i):
        return (z + Z - g) % Z * X + (x // 2 ^ u) * 2 + i

    def far(b, i):
        return remote(
            xs.at[cap_rows(2 * b + i), :],
            xb.at[y, pl.ds(b * CAP, CAP), :],
            a2a_s.at[0],
            a2a_r.at[b // 2],
            (there(*far_blocks[b], i), t),
        )

    def near(b, i):
        return remote(
            xsn.at[cap_rows(2 * b + i), :],
            xn.at[pl.ds(b * CAP, CAP), :],
            a2a_s.at[1],
            a2a_r.at[NF],
            (there(*near_blocks[b], i), t),
        )

    OWN = near_blocks.index((0, 0))

    def pick(group):
        row0 = slotrow[0:1, :].astype(jnp.int32)
        row1 = slotrow[1:2, :].astype(jnp.int32)
        parts = []
        for g, u in group:
            number = lax.broadcasted_iota(jnp.int32, (2 * CAP, T), 0) + there(g, u, 0) * CAP
            parts.append(jnp.where((number == row0) | (number == row1), 1.0, 0.0).astype(BF))
        return jnp.concatenate(parts, axis=0)

    @pl.when(active)
    def _():
        row0, row1 = slot_numbers()
        loads[0].wait()
        loads[11].wait()
        norm_routed()
        slotrow[0:1, :] = row0
        slotrow[1:2, :] = row1

        xs[...] = dot(pick(far_blocks), nrm[...]).astype(BF)

    @pl.when(jnp.logical_not(active))
    def _():
        for i in (0, 10, 11):
            loads[i].wait()

    pl.semaphore_wait(barrier, E + 2)

    @pl.when(active)
    def _():
        for b in range(len(far_blocks)):
            for i in range(2):
                far(b, i).start()

    weights = [
        remote(eg_hbm.at[0], wgu.at[:, pl.ds(FW, FW)], wt_s.at[0], wt_r.at[0], partner),
        remote(eu_hbm.at[0], wgu.at[:, pl.ds(3 * FW, FW)], wt_s.at[1], wt_r.at[1], partner),
        remote(ed_hbm.at[0], wd.at[pl.ds(FW, FW), :], wt_s.at[2], wt_r.at[2], partner),
        remote(wmo_hbm, wmo.at[pl.ds(HC, HC), :], wt_s.at[3], wt_r.at[3], partner),
    ]
    for one in weights:
        one.start()

    for i in (1, 2, 3, 4, 12, 13):
        loads[i].wait()

    def norm_mixer(i, carry):
        rows = pl.ds(pl.multiple_of(i * 16, 16), 16)
        v = mrows[rows, :].astype(F32)
        scale = lax.rsqrt(jnp.mean(v * v, axis=-1, keepdims=True) + EPS)
        mn[rows, :] = (v * scale * mgain[...]).astype(BF)
        return carry

    lax.fori_loop(0, M // 16, norm_mixer, 0)
    normed = mn[...]
    inner = dot_t(normed, win[...])
    gate_in = dot_t(normed, wgi[...])
    go[:, 0:HC] = dot_t(normed, wgo[...])
    ci[...] = jnp.zeros(ci.shape, BF)
    ci[:, 0:HC] = (gate_in * inner).astype(BF)
    send_halo = remote(ci.at[pl.ds(M - 16, 16), :], halo, halo_s, halo_r, ((c + 1) % E, t))
    send_halo.start()

    @pl.when(active)
    def _():
        def norm_full(i, carry):
            rows = pl.ds(pl.multiple_of(i * 16, 16), 16)
            v = rrows[rows, :].astype(F32)
            nfull[rows, :] = (v * rscale[rows, 0:1] * rgain[...]).astype(BF)
            return carry

        lax.fori_loop(0, T // 16, norm_full, 0)

        for first in range(0, len(near_blocks), 4):
            group = near_blocks[first : first + 4]
            rows = slice(2 * first * CAP, 2 * (first + len(group)) * CAP)
            xsn[rows, :] = dot(pick(group), nfull[...]).astype(BF)
        for b in range(len(near_blocks) - 1, -1, -1):
            for i in range(2):
                if b == OWN:
                    pl.when(x % 2 != i)(lambda: near(b, i).start())
                else:
                    near(b, i).start()
        xn[OWN * CAP : (OWN + 1) * CAP, :] = xsn[cap_rows(2 * OWN + x % 2), :]

        loads[10].wait()
        s0, s1, w0, w1 = slot_columns()
        s0 = s0.astype(jnp.int32)
        s1 = s1.astype(jnp.int32)
        for i in range(4):
            number = lax.broadcasted_iota(jnp.int32, (T, SC), 1) + i * SC
            w = jnp.where(number == s0, w0, 0.0) + jnp.where(number == s1, w1, 0.0)
            top = w.astype(BF)
            whi[:, i * SC : (i + 1) * SC] = top
            wlo[:, i * SC : (i + 1) * SC] = (w - top.astype(F32)).astype(BF)

    def ag_part(blk, d, s, q):
        if s < S:
            return xb.at[blk, pl.ds(q * QS, QS), :]
        return xb.at[blk, pl.ds(q * QS + d * (QS // 2), QS // 2), :]

    def ag(d, s, q, incoming):
        ref = ag_part((y + Y - sign[d] * (s if incoming else s - 1)) % Y, d, s, q)
        return remote(ref, ref, ag_s, ag_r.at[d, s - 1, q], ring[d])

    def gate_up(blk, rows=slice(None)):
        return dot(xb[blk, rows, :], wgu[pl.ds(pl.multiple_of(blk * CW, CW), CW), :])

    def near_arrived():
        @pl.when(active)
        def _():
            settle(xn.at[pl.ds(0, RN - CAP), :], a2a_r.at[NF])

        @pl.when(jnp.logical_not(active))
        def _():
            settle(xn, a2a_r.at[NF])

    def finish(both, rows):
        g = both[:, 0 : 2 * FW]
        hid[rows, :] = (g / (1.0 + jnp.exp(-g)) * both[:, 2 * FW :]).astype(BF)

    def columns_of(dest, half):
        return pl.ds(pl.multiple_of(dest * CW + half * CH, CH), CH)

    def mixer_partial(dest):
        cols = pl.ds(pl.multiple_of(dest * CW, CW), CW)
        mine = gsc[pl.ds(pl.multiple_of(k * MH, MH), MH), :]
        return dot(mine[:, 0:HC], wmo[0:HC, cols]) + dot(gpart[:, 0:HC], wmo[HC:, cols])

    def mx(d, s):
        rows = slice(d * MQ, (d + 1) * MQ) if s == 1 else slice(0, MH)
        rows = pl.ds(rows.start, rows.stop - rows.start)
        return remote(
            msbuf.at[d, s - 1, rows, :], mrbuf.at[d, s - 1, rows, :], mx_s, mx_r.at[d, s - 1], ring[d]
        )

    def mx_step(s):
        for d in range(2):
            b = mixer_partial((y + Y + sign[d] * (S + 1 - s)) % Y)
            msbuf[d, s - 1] = b.astype(BF)
            late = slice(d * MQ, (d + 1) * MQ)
            if s > 1:
                mx(d, s - 1).wait_recv()
                rows = late if s == 2 else slice(0, MH)
                msbuf[d, s - 1, rows, :] = (b[rows] + mrbuf[d, s - 2, rows, :].astype(F32)).astype(BF)
            mx(d, s).start()

    def mx_total():
        b = mixer_partial(y)
        for d in range(2):
            mx(d, S).wait_recv()
            b = b + mrbuf[d, S - 1].astype(F32)
        mout[pl.ds(pl.multiple_of(k * MH, MH), MH), cols_y] = b.astype(BF)

    mixer_steps = [functools.partial(mx_step, s) for s in range(1, S + 1)] + [mx_total]

    def mixer_on():
        if mixer_steps:
            mixer_steps.pop(0)()

    def partial(q, dest):
        return dot(hid[q % 2 * RH : (q % 2 + 1) * RH, :], wd[:, columns_of(dest, q // 2)])

    def slot(d, s, q):
        return d * 2 + q // 2 if s == 1 else 4 + ((s - 2) * 2 + d) * 4 + q

    def rs(d, s, q):
        i = slot(d, s, q)
        return remote(sbuf.at[i], rbuf.at[i], rs_s, rs_r.at[i], ring[d])

    def rs_step(d, s, q):
        a = partial(q, (y + Y + sign[d] * (S + 1 - s)) % Y)
        if s > 2 or (s == 2 and q % 2 == d):
            rs(d, s - 1, q).wait_recv()
            a = a + rbuf[slot(d, s - 1, q)].astype(F32)
        sbuf[slot(d, s, q)] = a.astype(BF)
        rs(d, s, q).start()

    def mixer_rest():
        send_halo.wait_recv()
        ext[0:16, :] = jnp.where(c > 0, halo[...].astype(F32), 0.0)
        ext[16:, :] = ci[...].astype(F32)
        conv = taps[0:1, :] * ext[14 : 14 + M, 0:HC]
        conv = conv + taps[1:2, :] * ext[15 : 15 + M, 0:HC]
        conv = conv + taps[2:3, :] * ext[16 : 16 + M, 0:HC]
        gsc[...] = jnp.zeros(gsc.shape, BF)
        gsc[:, 0:HC] = (go[:, 0:HC] * conv).astype(BF)
        send_g = remote(
            gsc.at[pl.ds(pl.multiple_of((1 - k) * MH, MH), MH), :], gpart, g_s, g_r, partner
        )
        send_g.start()
        return send_g

    def own_products():
        for i in (5, 6):
            loads[i].wait()
        weights[0].wait_recv()
        weights[1].wait_recv()
        acc[...] = gate_up(y)

    def products(rel):
        acc[...] += gate_up((y + Y + rel) % Y)

    hop = 2.75
    steps = [(s, q) for s in range(1, S + 1) for q in range(NF)]
    steps.sort(key=lambda one: (one[1] + hop * (one[0] - 1), -one[0]))
    waiting = []
    for s, q in steps:
        if s == 1:
            settle(xb.at[y, pl.ds(q * QS, QS), :], a2a_r.at[q])
        else:
            pass
        for d in range(2):
            if s > 1:
                ag(d, s - 1, q, True).wait_recv()
            ag(d, s, q, False).start()
        if q == NF - 1:
            waiting += [own_products] if s == 1 else [
                functools.partial(products, s - 1),
                functools.partial(products, 1 - s),
            ]
        if waiting:
            waiting.pop(0)()
        if (s, q) == (2, 0):
            send_g = mixer_rest()
            loads[8].wait()
        if (s, q) == (2, min(1, NF - 1)):
            weights[3].wait_recv()
            send_g.wait_recv()
        if (s, q) in ((2, min(1, NF - 1)), (3, 2), (4, 3)):
            mixer_on()
    for one in waiting:
        one()
    near_arrived()
    finish(dot(xn[...], wgu[...]), slice(0, RN))
    early = [(0, 1, 0), (1, 2, 0), (0, 1, 2), (1, 2, 2)]
    loads[7].wait()
    weights[2].wait_recv()
    for one in early:
        rs_step(*one)
    for q in range(NF):
        for d in range(2):
            ag(d, S, q, True).wait_recv()
    finish(acc[...] + gate_up((y + S) % Y), slice(RN, R))

    turns = [(0, 1), (1, 2), (2, 1), (3, 2)]
    for s in range(2, S):
        turns += [(0, s), (1, s + 1), (2, s), (3, s + 1)]
    turns += [(0, S), (2, S)]
    for n, (q, s) in enumerate(turns):
        for d in range(2):
            if (d, s, q ^ d) not in early:
                rs_step(d, s, q ^ d)
        if n in (1, 6):
            mixer_on()
    while mixer_steps:
        mixer_on()

    def mixer_piece(core, rel, h):
        cols = pl.ds(pl.multiple_of(((y + Y + rel) % Y) * CW, CW), CW)
        if h is None:
            return mout.at[pl.ds(pl.multiple_of(core * MH, MH), MH), cols]
        return mout.at[pl.ds(pl.multiple_of(core * MH + h * MQ, MQ), MQ), cols]

    def mg(d, j, incoming):
        h = None if j < S else d
        if incoming:
            ref = mixer_piece(k, -sign[d] * j, h)
        else:
            ref = mixer_piece(k, 0 if j <= 2 else -sign[d] * 2, h)
        dev = (c, ((y + Y + sign[d] * (j if j <= 2 else j - 2)) % Y) * 2 + k)
        return remote(ref, ref, mg_s, mg_r.at[d, j - 1], dev)

    def md(d, j):
        ref = mixer_piece(k, -sign[d] * j, None if j < S else d)
        return remote(ref, ref, md_s, md_r, partner)

    def mixer_arrived(j):
        for d in range(2):
            mg(d, j, True).wait_recv()
            if j == 2:
                for far_j in range(S, 2, -1):
                    mg(d, far_j, False).start()
            md(d, j).start()

    def target(i):
        g, u = blocks[i]
        return (z + g) % Z * X + (x // 2 ^ u) * 2 + k

    def giving(i, half):
        return remote(
            fin.at[half, pl.ds(i * CAP, CAP), :],
            ret.at[half, cap_rows(c), :],
            ret_s,
            ret_r.at[half],
            (target(i), t),
        )

    def distance(i):
        return min(blocks[i][0], Z - blocks[i][0])

    def unless_own(i, act):
        if i == OWN:
            pl.when(target(i) != c)(act)
        else:
            act()

    def total(q):
        a = partial(q, y)
        for d in range(2):
            rs(d, S, q).wait_recv()
            a = a + rbuf[slot(d, S, q)].astype(F32)
        half, rows = q // 2, q % 2
        fin[half, rows * RH : (rows + 1) * RH, :] = a.astype(BF)
        for i in sorted(range(rows * E // 4, (rows + 1) * E // 4), key=distance, reverse=True):
            unless_own(i, lambda: giving(i, half).start())

    total(0)
    total(1)

    total(2)
    total(3)
    for j in (2, 1):
        for d in range(2):
            mg(d, j, False).start()
    remote(mixer_piece(k, 0, None), mixer_piece(k, 0, None), md_s, md_r, partner).start()
    mixer_arrived(2)

    @pl.when(active)
    def _():
        for half in range(2):
            ret[half, cap_rows(c), :] = fin[half, OWN * CAP : (OWN + 1) * CAP, :]

    def routed_piece(rel, h):
        return rout.at[pl.ds(h % 2 * (T // 2), T // 2), columns_of((y + Y + rel) % Y, h // 2)]

    def pieces(j):
        return [(d, h) for h in range(4) for d in range(2) if j < S or h % 2 == d]

    via = [[0, 0, 0, 2, 2], [0, 0, 0, 2, 0]]

    def rg(d, j, h, incoming):
        last = via[h // 2][j]
        ref = routed_piece(-sign[d] * (j if incoming else last), h)
        dev = (c, ((y + Y + sign[d] * (j - last)) % Y) * 2 + k)
        return remote(ref, ref, rg_s, ag_r.at[d, j - 1, h], dev)

    def rd(d, j, h):
        ref = routed_piece(-sign[d] * j, h)
        return remote(ref, ref, rd_s, rd_r, partner)

    @pl.when(active)
    def _():
        for half in range(2):

            settle(ret.at[half, pl.ds(0, NS - CAP), :], ret_r.at[half])
            for h in range(2):
                rows = slice(h * (T // 2), (h + 1) * (T // 2))
                weighted = dot(whi[rows, :], ret[half]) + dot(wlo[rows, :], ret[half])
                rout[rows, columns_of(y, half)] = weighted.astype(BF)
                for j in (2, 4, 3, 1):
                    for d, i in pieces(j) if j <= S else []:
                        if i == 2 * half + h and via[half][j] == 0:
                            rg(d, j, i, False).start()
                rd(0, 0, 2 * half + h).start()
        due = [(half, j) for half, j in [(0, 2), (1, 2), (0, 1), (0, 3), (0, 4), (1, 1), (1, 4), (1, 3)] if j <= S]
        for n, (half, j) in enumerate(due):
            for d, h in pieces(j):
                if h // 2 == half:
                    rg(d, j, h, True).wait_recv()
                    for on in range(S, j, -1):
                        if via[half][on] == j and (d, h) in pieces(on):
                            rg(d, on, h, False).start()
                    rd(d, j, h).start()
            if n == 1:
                for m in [1] + list(range(3, S + 1)):
                    mixer_arrived(m)

    @pl.when(jnp.logical_not(active))
    def _():
        for j in [1] + list(range(3, S + 1)):
            mixer_arrived(j)

    settle(mout.at[pl.ds(0, MH), :], md_s)
    settle(mout.at[pl.ds(0, MH), :], md_r)
    settle(mout.at[pl.ds(0, MH), pl.ds(0, D - CW)], mg_s)
    settle(mout.at[pl.ds(0, MH), pl.ds(0, D - CW)], mx_s)
    settle(xb.at[pl.ds(0, Y - 1)], ag_s)
    settle(sbuf, rs_s)
    for one in weights:
        one.wait_send()
    send_halo.wait_send()
    send_g.wait_send()
    @pl.when(active)
    def _():
        settle(fin.at[:, pl.ds(0, R - CAP), :], ret_s)
        settle(xs, a2a_s.at[0])
        settle(xsn.at[pl.ds(0, 2 * RN - CAP), :], a2a_s.at[1])
        settle(rout.at[:, pl.ds(0, D - CW)], rg_s)
        settle(rout, rd_s)

    @pl.when(jnp.logical_not(active))
    def _():
        settle(fin, ret_s)
        settle(rout, rd_r)


def put(a, b, out_a, out_b, same_a, same_b, sem):
    copies = [
        pltpu.make_async_copy(a, out_a, sem.at[0]),
        pltpu.make_async_copy(b, out_b, sem.at[1]),
    ]
    for one in copies:
        one.start()
    for one in copies:
        one.wait()


def on_device(E, Y, mrows, mgain, win, wgi, wgo, taps, wmo, rrows, rgain, ids, rw, eg, eu, ed):
    M, D = mrows.shape
    T = rrows.shape[0]
    HC = win.shape[1]
    FW = eg.shape[2]
    CW = D // Y
    S = Y // 2
    CAP = 2 * T * ids.shape[1] // E
    X = 4
    near_blocks, far_blocks = plan(E // X)
    NF = len(far_blocks) // 2
    R = E * CAP // 2
    RN = len(near_blocks) * CAP
    VM = pl.BlockSpec(memory_space=pltpu.VMEM)
    HB = pl.BlockSpec(memory_space=pl.ANY)
    DS = pltpu.SemaphoreType.DMA
    results = pl.pallas_call(
        functools.partial(kernel, E, Y, X, CAP),
        out_shape=(pltpu.VMEM((M, D), BF), pltpu.VMEM((T, D), BF)),
        in_specs=[HB] * 14,
        out_specs=(VM, VM),
        scratch_shapes=[
            pltpu.VMEM((1, D), F32),
            pltpu.VMEM(taps.shape, F32),
            pltpu.VMEM((1, D), F32),
            pltpu.VMEM((2, T), jnp.int32),
            pltpu.VMEM((2, T), F32),
            pltpu.VMEM((M, D), BF),
            pltpu.VMEM((M, D), BF),
            pltpu.VMEM((HC, D), BF),
            pltpu.VMEM((HC, D), BF),
            pltpu.VMEM((HC, D), BF),
            pltpu.VMEM((2 * HC, D), BF),
            pltpu.VMEM((T, D), BF),
            pltpu.VMEM((T, CW), BF),
            pltpu.VMEM((T, D), BF),
            pltpu.VMEM((T, 128), F32),
            pltpu.VMEM((D, 4 * FW), BF),
            pltpu.VMEM((2 * FW, D), BF),
            pltpu.VMEM((8, T), F32),
            pltpu.VMEM(((R - RN) * 2, CW), BF),
            pltpu.VMEM((2 * RN, D), BF),
            pltpu.VMEM((Y, R - RN, CW), BF),
            pltpu.VMEM((RN, D), BF),
            pltpu.VMEM((R - RN, 4 * FW), F32),
            pltpu.VMEM((R, 2 * FW), BF),
            pltpu.VMEM((8 * S - 4, R // 2, CW // 2), BF),
            pltpu.VMEM((8 * S - 4, R // 2, CW // 2), BF),
            pltpu.VMEM((2, S, M // 2, CW), BF),
            pltpu.VMEM((2, S, M // 2, CW), BF),
            pltpu.VMEM((2, R, CW // 2), BF),
            pltpu.VMEM((2, E * CAP, CW // 2), BF),
            pltpu.VMEM((T, E * CAP), BF),
            pltpu.VMEM((T, E * CAP), BF),
            pltpu.VMEM((M, 128), BF),
            pltpu.VMEM((16, 128), BF),
            pltpu.VMEM((M + 16, 128), F32),
            pltpu.VMEM((M, 128), F32),
            pltpu.VMEM((M, 128), BF),
            pltpu.VMEM((M // 2, 128), BF),
            DS((14,)),
            DS((4,)),
            DS((4,)),
            DS((2,)),
            DS((NF + 1,)),
            DS,
            DS,
            DS,
            DS,
            DS,
            DS((2, S, max(NF, 4))),
            DS,
            DS((8 * S - 4,)),
            DS,
            DS((2, S)),
            DS,
            DS((2,)),
            DS,
            DS((2, S)),
            DS,
            DS,
            DS,
            DS,
            DS,
        ],
        compiler_params=pltpu.CompilerParams(collective_id=0, has_side_effects=True),
    )(
        mrows,
        mgain.reshape(1, D),
        win.T,
        wgi.T,
        wgo.T,
        taps,
        wmo,
        rrows,
        rgain.reshape(1, D),
        ids.T,
        rw.T,
        eg,
        eu,
        ed,
    )
    return pl.pallas_call(
        put,
        out_shape=(
            jax.ShapeDtypeStruct((M, D), BF),
            jax.ShapeDtypeStruct((T, D), BF),
            pltpu.VMEM((M, D), BF),
            pltpu.VMEM((T, D), BF),
        ),
        in_specs=[VM, VM],
        out_specs=(HB, HB, VM, VM),
        scratch_shapes=[DS((2,))],
        input_output_aliases={0: 2, 1: 3},
    )(*results)[:2]


def solution(mesh):
    E = mesh.shape["ep"]
    Y = mesh.shape["tp"] // 2
    return jax.shard_map(
        functools.partial(on_device, E, Y),
        mesh=mesh,
        in_specs=(
            P("ep", None),
            P(),
            P(None, "tp"),
            P(None, "tp"),
            P(None, "tp"),
            P(None, "tp"),
            P("tp", None),
            P("ep", None),
            P(),
            P("ep", None),
            P("ep", None),
            P("ep", None, "tp"),
            P("ep", None, "tp"),
            P("ep", "tp", None),
        ),
        out_specs=(P("ep", None), P("ep", None)),
        check_vma=False,
    )
```

```python
import functools

import jax
import jax.numpy as jnp
from jax import lax
from jax.experimental import pallas as pl
from jax.experimental.pallas import tpu as pltpu
from jax.sharding import PartitionSpec as P

MESH = pl.DeviceIdType.MESH
BF = jnp.bfloat16
F32 = jnp.float32
EPS = 1e-06


def dot(a, b):
    return jnp.dot(a, b, preferred_element_type=F32)


def plan(Z):
    every = [(g, u) for g in sorted(range(Z), key=lambda g: min(g, Z - g)) for u in range(2)]
    reach = 1 if Z > 4 else 0
    near = [b for b in every if min(b[0], Z - b[0]) <= reach]
    if reach:
        near += [(2, 0), (Z - 2, 0)]
    return near, sorted([b for b in every if b not in near], key=lambda b: min(b[0], Z - b[0]))


def dot_t(a, b):
    return lax.dot_general(a, b, (((1,), (1,)), ((), ())), preferred_element_type=F32)


def kernel(
    E,
    Y,
    X,
    CAP,
    mrows_hbm,
    mgain_hbm,
    win_hbm,
    wgi_hbm,
    wgo_hbm,
    taps_hbm,
    wmo_hbm,
    rrows_hbm,
    rgain_hbm,
    ids_hbm,
    rw_hbm,
    eg_hbm,
    eu_hbm,
    ed_hbm,
    mout,
    rout,
    mgain,
    taps,
    rgain,
    ids_ref,
    rw_ref,
    mrows,
    mn,
    win,
    wgi,
    wgo,
    wmo,
    rrows,
    nrm,
    nfull,
    rscale,
    wgu,
    wd,
    slotrow,
    xs,
    xsn,
    xb,
    xn,
    acc,
    hid,
    sbuf,
    rbuf,
    msbuf,
    mrbuf,
    fin,
    ret,
    whi,
    wlo,
    ci,
    halo,
    ext,
    go,
    gsc,
    gpart,
    l_sem,
    wt_s,
    wt_r,
    a2a_s,
    a2a_r,
    halo_s,
    halo_r,
    g_s,
    g_r,
    ag_s,
    ag_r,
    rs_s,
    rs_r,
    mx_s,
    mx_r,
    ret_s,
    ret_r,
    mg_s,
    mg_r,
    md_s,
    md_r,
    rg_s,
    rd_s,
    rd_r,
):
    S = Y // 2
    c = lax.axis_index("ep")
    t = lax.axis_index("tp")
    y = t // 2
    k = t % 2
    z = c // X
    x = c % X
    active = k == c % 2
    M, D = mn.shape
    T = nrm.shape[0]
    CW = D // Y
    NS = E * CAP
    R = NS // 2
    Z = E // X
    near_blocks, far_blocks = plan(Z)
    blocks = near_blocks + far_blocks
    NF = len(far_blocks) // 2
    RN = len(near_blocks) * CAP
    RF = len(far_blocks) * CAP
    QS = 2 * CAP
    RH = R // 2
    CH = CW // 2
    MH = M // 2
    MQ = MH // 2
    HC = win.shape[0]
    EP = -(-E // 16) * 16
    partner = (c, y * 2 + 1 - k)
    ring = [(c, ((y + 1) % Y) * 2 + k), (c, ((y + Y - 1) % Y) * 2 + k)]
    sign = [1, -1]

    def remote(src, dst, ss, rs, dev):
        return pltpu.make_async_remote_copy(
            src_ref=src, dst_ref=dst, send_sem=ss, recv_sem=rs, device_id=dev, device_id_type=MESH
        )

    def settle(ref, sem):
        pltpu.make_async_copy(ref, ref, sem).wait()

    FW = eg_hbm.shape[2]
    loads = [
        pltpu.make_async_copy(
            rrows_hbm.at[pl.ds(0, T // 2), :], rrows.at[pl.ds(0, T // 2), :], l_sem.at[0]
        ),
        pltpu.make_async_copy(mrows_hbm, mrows, l_sem.at[1]),
        pltpu.make_async_copy(win_hbm, win, l_sem.at[2]),
        pltpu.make_async_copy(wgi_hbm, wgi, l_sem.at[3]),
        pltpu.make_async_copy(wgo_hbm, wgo, l_sem.at[4]),
        pltpu.make_async_copy(eg_hbm.at[0], wgu.at[:, pl.ds(0, FW)], l_sem.at[5]),
        pltpu.make_async_copy(eu_hbm.at[0], wgu.at[:, pl.ds(2 * FW, FW)], l_sem.at[6]),
        pltpu.make_async_copy(ed_hbm.at[0], wd.at[pl.ds(0, FW), :], l_sem.at[7]),
        pltpu.make_async_copy(wmo_hbm, wmo.at[pl.ds(0, HC), :], l_sem.at[8]),
        pltpu.make_async_copy(ids_hbm, ids_ref, l_sem.at[9]),
        pltpu.make_async_copy(rw_hbm, rw_ref, l_sem.at[10]),
        pltpu.make_async_copy(rgain_hbm, rgain, l_sem.at[11]),
        pltpu.make_async_copy(mgain_hbm, mgain, l_sem.at[12]),
        pltpu.make_async_copy(taps_hbm, taps, l_sem.at[13]),
        pltpu.make_async_copy(
            rrows_hbm.at[pl.ds(T // 2, T // 2), :], rrows.at[pl.ds(T // 2, T // 2), :], l_sem.at[14]
        ),
    ]
    for i in (9, 0, 11, 14):
        loads[i].start()

    barrier = pltpu.get_barrier_semaphore()

    for g in sorted(range(Z), key=lambda g: -min(g, Z - g)):

        def greet(i, carry):
            there = (z + g) % Z * X + (x + i) % X
            pl.semaphore_signal(barrier, inc=1, device_id=(there, t), device_id_type=MESH)
            return carry

        lax.fori_loop(0 if g else 1, X, greet, 0)
    for dev in (partner, ring[0], ring[1]):
        pl.semaphore_signal(barrier, inc=1, device_id=dev, device_id_type=MESH)

    for i in (1, 12, 2, 3, 4, 10, 13, 5, 6, 7, 8):
        loads[i].start()

    def slot_numbers():
        ids = ids_ref[...]
        expert = lax.broadcasted_iota(jnp.int32, (EP, T), 0)
        hit0 = expert == ids[0:1, :]
        hit1 = expert == ids[1:2, :]
        named = jnp.where(hit0 | hit1, 1.0, 0.0).astype(BF)
        r = lax.broadcasted_iota(jnp.int32, (T, T), 0)
        q = lax.broadcasted_iota(jnp.int32, (T, T), 1)
        upper = jnp.where(r < q, 1.0, 0.0).astype(BF)
        before = dot(named, upper)
        row0 = ids[0:1, :].astype(F32) * CAP + jnp.sum(
            jnp.where(hit0, before, 0.0), axis=0, keepdims=True
        )
        row1 = ids[1:2, :].astype(F32) * CAP + jnp.sum(
            jnp.where(hit1, before, 0.0), axis=0, keepdims=True
        )
        return row0, row1

    def slot_columns():
        r = lax.broadcasted_iota(jnp.int32, (T, T), 0)
        q = lax.broadcasted_iota(jnp.int32, (T, T), 1)
        diag = r == q
        rows = (slotrow[0:1, :], slotrow[1:2, :], rw_ref[0:1, :], rw_ref[1:2, :])
        return [jnp.sum(jnp.where(diag, row, 0.0), axis=1, keepdims=True) for row in rows]

    cols_y = pl.ds(pl.multiple_of(y * CW, CW), CW)

    def norm_routed():
        step = 32

        def body(i, carry):
            rows = pl.ds(pl.multiple_of(i * step, step), step)
            v = rrows[rows, :].astype(F32)
            scale = lax.rsqrt(jnp.mean(v * v, axis=-1, keepdims=True) + EPS)
            rscale[rows, :] = jnp.broadcast_to(scale, (step, 128))
            part = rrows[rows, cols_y].astype(F32)
            nrm[rows, :] = (part * scale * rgain[:, cols_y]).astype(BF)
            return carry

        lax.fori_loop(0, T // step // 2, body, 0)
        loads[14].wait()
        lax.fori_loop(T // step // 2, T // step, body, 0)

    loads[9].wait()

    SC = NS // 4

    def cap_rows(i):
        return pl.ds(pl.multiple_of(i * CAP, CAP), CAP)

    def there(g, u, i):
        return (z + Z - g) % Z * X + (x // 2 ^ u) * 2 + i

    def far(b, i):
        return remote(
            xs.at[cap_rows(2 * b + i), :],
            xb.at[y, pl.ds(b * CAP, CAP), :],
            a2a_s.at[0],
            a2a_r.at[b // 2],
            (there(*far_blocks[b], i), t),
        )

    def near(b, i):
        return remote(
            xsn.at[cap_rows(2 * b + i), :],
            xn.at[pl.ds(b * CAP, CAP), :],
            a2a_s.at[1],
            a2a_r.at[NF],
            (there(*near_blocks[b], i), t),
        )

    OWN = near_blocks.index((0, 0))

    def pick(group):
        row0 = slotrow[0:1, :].astype(jnp.int32)
        row1 = slotrow[1:2, :].astype(jnp.int32)
        parts = []
        for g, u in group:
            number = lax.broadcasted_iota(jnp.int32, (2 * CAP, T), 0) + there(g, u, 0) * CAP
            parts.append(jnp.where((number == row0) | (number == row1), 1.0, 0.0).astype(BF))
        return jnp.concatenate(parts, axis=0)

    @pl.when(active)
    def _():
        row0, row1 = slot_numbers()
        loads[0].wait()
        loads[11].wait()
        norm_routed()
        slotrow[0:1, :] = row0
        slotrow[1:2, :] = row1

        xs[...] = dot(pick(far_blocks), nrm[...]).astype(BF)

    @pl.when(jnp.logical_not(active))
    def _():
        for i in (0, 10, 11, 14):
            loads[i].wait()

    pl.semaphore_wait(barrier, E + 2)

    @pl.when(active)
    def _():
        for b in range(len(far_blocks)):
            for i in range(2):
                far(b, i).start()

    weights = [
        remote(eg_hbm.at[0], wgu.at[:, pl.ds(FW, FW)], wt_s.at[0], wt_r.at[0], partner),
        remote(eu_hbm.at[0], wgu.at[:, pl.ds(3 * FW, FW)], wt_s.at[1], wt_r.at[1], partner),
        remote(ed_hbm.at[0], wd.at[pl.ds(FW, FW), :], wt_s.at[2], wt_r.at[2], partner),
        remote(wmo_hbm, wmo.at[pl.ds(HC, HC), :], wt_s.at[3], wt_r.at[3], partner),
    ]
    for one in weights:
        one.start()

    for i in (1, 2, 3, 4, 12, 13):
        loads[i].wait()

    def norm_mixer(i, carry):
        rows = pl.ds(pl.multiple_of(i * 16, 16), 16)
        v = mrows[rows, :].astype(F32)
        scale = lax.rsqrt(jnp.mean(v * v, axis=-1, keepdims=True) + EPS)
        mn[rows, :] = (v * scale * mgain[...]).astype(BF)
        return carry

    lax.fori_loop(0, M // 16, norm_mixer, 0)
    normed = mn[...]
    inner = dot_t(normed, win[...])
    gate_in = dot_t(normed, wgi[...])
    go[:, 0:HC] = dot_t(normed, wgo[...])
    ci[...] = jnp.zeros(ci.shape, BF)
    ci[:, 0:HC] = (gate_in * inner).astype(BF)
    send_halo = remote(ci.at[pl.ds(M - 16, 16), :], halo, halo_s, halo_r, ((c + 1) % E, t))
    send_halo.start()

    @pl.when(active)
    def _():
        def norm_full(i, carry):
            rows = pl.ds(pl.multiple_of(i * 16, 16), 16)
            v = rrows[rows, :].astype(F32)
            nfull[rows, :] = (v * rscale[rows, 0:1] * rgain[...]).astype(BF)
            return carry

        lax.fori_loop(0, T // 16, norm_full, 0)

        for first in range(0, len(near_blocks), 4):
            group = near_blocks[first : first + 4]
            rows = slice(2 * first * CAP, 2 * (first + len(group)) * CAP)
            xsn[rows, :] = dot(pick(group), nfull[...]).astype(BF)
        for b in range(len(near_blocks) - 1, -1, -1):
            for i in range(2):
                if b == OWN:
                    pl.when(x % 2 != i)(lambda: near(b, i).start())
                else:
                    near(b, i).start()
        xn[OWN * CAP : (OWN + 1) * CAP, :] = xsn[cap_rows(2 * OWN + x % 2), :]

        loads[10].wait()
        s0, s1, w0, w1 = slot_columns()
        s0 = s0.astype(jnp.int32)
        s1 = s1.astype(jnp.int32)
        for i in range(4):
            number = lax.broadcasted_iota(jnp.int32, (T, SC), 1) + i * SC
            w = jnp.where(number == s0, w0, 0.0) + jnp.where(number == s1, w1, 0.0)
            top = w.astype(BF)
            whi[:, i * SC : (i + 1) * SC] = top
            wlo[:, i * SC : (i + 1) * SC] = (w - top.astype(F32)).astype(BF)

    def ag_part(blk, d, s, q):
        if s < S:
            return xb.at[blk, pl.ds(q * QS, QS), :]
        return xb.at[blk, pl.ds(q * QS + d * (QS // 2), QS // 2), :]

    def ag(d, s, q, incoming):
        ref = ag_part((y + Y - sign[d] * (s if incoming else s - 1)) % Y, d, s, q)
        return remote(ref, ref, ag_s, ag_r.at[d, s - 1, q], ring[d])

    def gate_up(blk, rows=slice(None)):
        return dot(xb[blk, rows, :], wgu[pl.ds(pl.multiple_of(blk * CW, CW), CW), :])

    def near_arrived():
        @pl.when(active)
        def _():
            settle(xn.at[pl.ds(0, RN - CAP), :], a2a_r.at[NF])

        @pl.when(jnp.logical_not(active))
        def _():
            settle(xn, a2a_r.at[NF])

    def finish(both, rows):
        g = both[:, 0 : 2 * FW]
        hid[rows, :] = (g / (1.0 + jnp.exp(-g)) * both[:, 2 * FW :]).astype(BF)

    def columns_of(dest, half):
        return pl.ds(pl.multiple_of(dest * CW + half * CH, CH), CH)

    def mixer_partial(dest):
        cols = pl.ds(pl.multiple_of(dest * CW, CW), CW)
        mine = gsc[pl.ds(pl.multiple_of(k * MH, MH), MH), :]
        return dot(mine[:, 0:HC], wmo[0:HC, cols]) + dot(gpart[:, 0:HC], wmo[HC:, cols])

    def mx(d, s):
        rows = slice(d * MQ, (d + 1) * MQ) if s == 1 else slice(0, MH)
        rows = pl.ds(rows.start, rows.stop - rows.start)
        return remote(
            msbuf.at[d, s - 1, rows, :], mrbuf.at[d, s - 1, rows, :], mx_s, mx_r.at[d, s - 1], ring[d]
        )

    def mx_step(s):
        for d in range(2):
            b = mixer_partial((y + Y + sign[d] * (S + 1 - s)) % Y)
            msbuf[d, s - 1] = b.astype(BF)
            late = slice(d * MQ, (d + 1) * MQ)
            if s > 1:
                mx(d, s - 1).wait_recv()
                rows = late if s == 2 else slice(0, MH)
                msbuf[d, s - 1, rows, :] = (b[rows] + mrbuf[d, s - 2, rows, :].astype(F32)).astype(BF)
            mx(d, s).start()

    def mx_total():
        b = mixer_partial(y)
        for d in range(2):
            mx(d, S).wait_recv()
            b = b + mrbuf[d, S - 1].astype(F32)
        mout[pl.ds(pl.multiple_of(k * MH, MH), MH), cols_y] = b.astype(BF)

    mixer_steps = [functools.partial(mx_step, s) for s in range(1, S + 1)] + [mx_total]

    def mixer_on():
        if mixer_steps:
            mixer_steps.pop(0)()

    def partial(q, dest):
        return dot(hid[q % 2 * RH : (q % 2 + 1) * RH, :], wd[:, columns_of(dest, q // 2)])

    def slot(d, s, q):
        return d * 2 + q // 2 if s == 1 else 4 + ((s - 2) * 2 + d) * 4 + q

    def rs(d, s, q):
        i = slot(d, s, q)
        return remote(sbuf.at[i], rbuf.at[i], rs_s, rs_r.at[i], ring[d])

    def rs_step(d, s, q):
        a = partial(q, (y + Y + sign[d] * (S + 1 - s)) % Y)
        if s > 2 or (s == 2 and q % 2 == d):
            rs(d, s - 1, q).wait_recv()
            a = a + rbuf[slot(d, s - 1, q)].astype(F32)
        sbuf[slot(d, s, q)] = a.astype(BF)
        rs(d, s, q).start()

    def mixer_rest():
        send_halo.wait_recv()
        ext[0:16, :] = jnp.where(c > 0, halo[...].astype(F32), 0.0)
        ext[16:, :] = ci[...].astype(F32)
        conv = taps[0:1, :] * ext[14 : 14 + M, 0:HC]
        conv = conv + taps[1:2, :] * ext[15 : 15 + M, 0:HC]
        conv = conv + taps[2:3, :] * ext[16 : 16 + M, 0:HC]
        gsc[...] = jnp.zeros(gsc.shape, BF)
        gsc[:, 0:HC] = (go[:, 0:HC] * conv).astype(BF)
        send_g = remote(
            gsc.at[pl.ds(pl.multiple_of((1 - k) * MH, MH), MH), :], gpart, g_s, g_r, partner
        )
        send_g.start()
        return send_g

    def own_products():
        for i in (5, 6):
            loads[i].wait()
        weights[0].wait_recv()
        weights[1].wait_recv()
        acc[...] = gate_up(y)

    def products(rel):
        acc[...] += gate_up((y + Y + rel) % Y)

    hop = 2.75
    steps = [(s, q) for s in range(1, S + 1) for q in range(NF)]
    steps.sort(key=lambda one: (one[1] + hop * (one[0] - 1), -one[0]))
    waiting = []
    for s, q in steps:
        if s == 1:
            settle(xb.at[y, pl.ds(q * QS, QS), :], a2a_r.at[q])
        else:
            pass
        for d in range(2):
            if s > 1:
                ag(d, s - 1, q, True).wait_recv()
            ag(d, s, q, False).start()
        if q == NF - 1:
            waiting += [own_products] if s == 1 else [
                functools.partial(products, s - 1),
                functools.partial(products, 1 - s),
            ]
        if waiting:
            waiting.pop(0)()
        if (s, q) == (2, 0):
            send_g = mixer_rest()
            loads[8].wait()
        if (s, q) == (2, min(1, NF - 1)):
            weights[3].wait_recv()
            send_g.wait_recv()
        if (s, q) in ((2, min(1, NF - 1)), (3, 2), (4, 3)):
            mixer_on()
    for one in waiting:
        one()
    near_arrived()
    finish(dot(xn[...], wgu[...]), slice(0, RN))
    early = [(0, 1, 0), (1, 2, 0), (0, 1, 2), (1, 2, 2)]
    loads[7].wait()
    weights[2].wait_recv()
    for one in early:
        rs_step(*one)
    for q in range(NF):
        for d in range(2):
            ag(d, S, q, True).wait_recv()
    finish(acc[...] + gate_up((y + S) % Y), slice(RN, R))

    turns = [(0, 1), (1, 2), (2, 1), (3, 2)]
    for s in range(2, S):
        turns += [(0, s), (1, s + 1), (2, s), (3, s + 1)]
    turns += [(0, S), (2, S)]
    for n, (q, s) in enumerate(turns):
        for d in range(2):
            if (d, s, q ^ d) not in early:
                rs_step(d, s, q ^ d)
        if n in (1, 6):
            mixer_on()
    while mixer_steps:
        mixer_on()

    def mixer_piece(core, rel, h):
        cols = pl.ds(pl.multiple_of(((y + Y + rel) % Y) * CW, CW), CW)
        if h is None:
            return mout.at[pl.ds(pl.multiple_of(core * MH, MH), MH), cols]
        return mout.at[pl.ds(pl.multiple_of(core * MH + h * MQ, MQ), MQ), cols]

    def mg(d, j, incoming):
        h = None if j < S else d
        if incoming:
            ref = mixer_piece(k, -sign[d] * j, h)
        else:
            ref = mixer_piece(k, 0 if j <= 2 else -sign[d] * 2, h)
        dev = (c, ((y + Y + sign[d] * (j if j <= 2 else j - 2)) % Y) * 2 + k)
        return remote(ref, ref, mg_s, mg_r.at[d, j - 1], dev)

    def md(d, j):
        ref = mixer_piece(k, -sign[d] * j, None if j < S else d)
        return remote(ref, ref, md_s, md_r, partner)

    def mixer_arrived(j):
        for d in range(2):
            mg(d, j, True).wait_recv()
            if j == 2:
                for far_j in range(S, 2, -1):
                    mg(d, far_j, False).start()
            md(d, j).start()

    def target(i):
        g, u = blocks[i]
        return (z + g) % Z * X + (x // 2 ^ u) * 2 + k

    def giving(i, half):
        return remote(
            fin.at[half, pl.ds(i * CAP, CAP), :],
            ret.at[half, cap_rows(c), :],
            ret_s,
            ret_r.at[half],
            (target(i), t),
        )

    def distance(i):
        return min(blocks[i][0], Z - blocks[i][0])

    def unless_own(i, act):
        if i == OWN:
            pl.when(target(i) != c)(act)
        else:
            act()

    def total(q):
        a = partial(q, y)
        for d in range(2):
            rs(d, S, q).wait_recv()
            a = a + rbuf[slot(d, S, q)].astype(F32)
        half, rows = q // 2, q % 2
        fin[half, rows * RH : (rows + 1) * RH, :] = a.astype(BF)
        for i in sorted(range(rows * E // 4, (rows + 1) * E // 4), key=distance, reverse=True):
            unless_own(i, lambda: giving(i, half).start())

    total(0)
    total(1)

    total(2)
    total(3)
    for j in (2, 1):
        for d in range(2):
            mg(d, j, False).start()
    remote(mixer_piece(k, 0, None), mixer_piece(k, 0, None), md_s, md_r, partner).start()
    mixer_arrived(2)

    @pl.when(active)
    def _():
        for half in range(2):
            ret[half, cap_rows(c), :] = fin[half, OWN * CAP : (OWN + 1) * CAP, :]

    def routed_piece(rel, h):
        return rout.at[pl.ds(h % 2 * (T // 2), T // 2), columns_of((y + Y + rel) % Y, h // 2)]

    def pieces(j):
        return [(d, h) for h in range(4) for d in range(2) if j < S or h % 2 == d]

    via = [[0, 0, 0, 2, 2], [0, 0, 0, 2, 0]]

    def rg(d, j, h, incoming):
        last = via[h // 2][j]
        ref = routed_piece(-sign[d] * (j if incoming else last), h)
        dev = (c, ((y + Y + sign[d] * (j - last)) % Y) * 2 + k)
        return remote(ref, ref, rg_s, ag_r.at[d, j - 1, h], dev)

    def rd(d, j, h):
        ref = routed_piece(-sign[d] * j, h)
        return remote(ref, ref, rd_s, rd_r, partner)

    @pl.when(active)
    def _():
        for half in range(2):

            settle(ret.at[half, pl.ds(0, NS - CAP), :], ret_r.at[half])
            for h in range(2):
                rows = slice(h * (T // 2), (h + 1) * (T // 2))
                weighted = dot(whi[rows, :], ret[half]) + dot(wlo[rows, :], ret[half])
                rout[rows, columns_of(y, half)] = weighted.astype(BF)
                for j in (2, 4, 3, 1):
                    for d, i in pieces(j) if j <= S else []:
                        if i == 2 * half + h and via[half][j] == 0:
                            rg(d, j, i, False).start()
                rd(0, 0, 2 * half + h).start()
        due = [(half, j) for half, j in [(0, 2), (1, 2), (0, 1), (0, 3), (0, 4), (1, 1), (1, 4), (1, 3)] if j <= S]
        for n, (half, j) in enumerate(due):
            for d, h in pieces(j):
                if h // 2 == half:
                    rg(d, j, h, True).wait_recv()
                    for on in range(S, j, -1):
                        if via[half][on] == j and (d, h) in pieces(on):
                            rg(d, on, h, False).start()
                    rd(d, j, h).start()
            if n == 1:
                for m in [1] + list(range(3, S + 1)):
                    mixer_arrived(m)

    @pl.when(jnp.logical_not(active))
    def _():
        for j in [1] + list(range(3, S + 1)):
            mixer_arrived(j)

    settle(mout.at[pl.ds(0, MH), :], md_s)
    settle(mout.at[pl.ds(0, MH), :], md_r)
    settle(mout.at[pl.ds(0, MH), pl.ds(0, D - CW)], mg_s)
    settle(mout.at[pl.ds(0, MH), pl.ds(0, D - CW)], mx_s)
    settle(xb.at[pl.ds(0, Y - 1)], ag_s)
    settle(sbuf, rs_s)
    for one in weights:
        one.wait_send()
    send_halo.wait_send()
    send_g.wait_send()
    @pl.when(active)
    def _():
        settle(fin.at[:, pl.ds(0, R - CAP), :], ret_s)
        settle(xs, a2a_s.at[0])
        settle(xsn.at[pl.ds(0, 2 * RN - CAP), :], a2a_s.at[1])
        settle(rout.at[:, pl.ds(0, D - CW)], rg_s)
        settle(rout, rd_s)

    @pl.when(jnp.logical_not(active))
    def _():
        settle(fin, ret_s)
        settle(rout, rd_r)


def put(a, b, out_a, out_b, same_a, same_b, sem):
    copies = [
        pltpu.make_async_copy(a, out_a, sem.at[0]),
        pltpu.make_async_copy(b, out_b, sem.at[1]),
    ]
    for one in copies:
        one.start()
    for one in copies:
        one.wait()


def on_device(E, Y, mrows, mgain, win, wgi, wgo, taps, wmo, rrows, rgain, ids, rw, eg, eu, ed):
    M, D = mrows.shape
    T = rrows.shape[0]
    HC = win.shape[1]
    FW = eg.shape[2]
    CW = D // Y
    S = Y // 2
    CAP = 2 * T * ids.shape[1] // E
    X = 4
    near_blocks, far_blocks = plan(E // X)
    NF = len(far_blocks) // 2
    R = E * CAP // 2
    RN = len(near_blocks) * CAP
    VM = pl.BlockSpec(memory_space=pltpu.VMEM)
    HB = pl.BlockSpec(memory_space=pl.ANY)
    DS = pltpu.SemaphoreType.DMA
    results = pl.pallas_call(
        functools.partial(kernel, E, Y, X, CAP),
        out_shape=(pltpu.VMEM((M, D), BF), pltpu.VMEM((T, D), BF)),
        in_specs=[HB] * 14,
        out_specs=(VM, VM),
        scratch_shapes=[
            pltpu.VMEM((1, D), F32),
            pltpu.VMEM(taps.shape, F32),
            pltpu.VMEM((1, D), F32),
            pltpu.VMEM((2, T), jnp.int32),
            pltpu.VMEM((2, T), F32),
            pltpu.VMEM((M, D), BF),
            pltpu.VMEM((M, D), BF),
            pltpu.VMEM((HC, D), BF),
            pltpu.VMEM((HC, D), BF),
            pltpu.VMEM((HC, D), BF),
            pltpu.VMEM((2 * HC, D), BF),
            pltpu.VMEM((T, D), BF),
            pltpu.VMEM((T, CW), BF),
            pltpu.VMEM((T, D), BF),
            pltpu.VMEM((T, 128), F32),
            pltpu.VMEM((D, 4 * FW), BF),
            pltpu.VMEM((2 * FW, D), BF),
            pltpu.VMEM((8, T), F32),
            pltpu.VMEM(((R - RN) * 2, CW), BF),
            pltpu.VMEM((2 * RN, D), BF),
            pltpu.VMEM((Y, R - RN, CW), BF),
            pltpu.VMEM((RN, D), BF),
            pltpu.VMEM((R - RN, 4 * FW), F32),
            pltpu.VMEM((R, 2 * FW), BF),
            pltpu.VMEM((8 * S - 4, R // 2, CW // 2), BF),
            pltpu.VMEM((8 * S - 4, R // 2, CW // 2), BF),
            pltpu.VMEM((2, S, M // 2, CW), BF),
            pltpu.VMEM((2, S, M // 2, CW), BF),
            pltpu.VMEM((2, R, CW // 2), BF),
            pltpu.VMEM((2, E * CAP, CW // 2), BF),
            pltpu.VMEM((T, E * CAP), BF),
            pltpu.VMEM((T, E * CAP), BF),
            pltpu.VMEM((M, 128), BF),
            pltpu.VMEM((16, 128), BF),
            pltpu.VMEM((M + 16, 128), F32),
            pltpu.VMEM((M, 128), F32),
            pltpu.VMEM((M, 128), BF),
            pltpu.VMEM((M // 2, 128), BF),
            DS((15,)),
            DS((4,)),
            DS((4,)),
            DS((2,)),
            DS((NF + 1,)),
            DS,
            DS,
            DS,
            DS,
            DS,
            DS((2, S, max(NF, 4))),
            DS,
            DS((8 * S - 4,)),
            DS,
            DS((2, S)),
            DS,
            DS((2,)),
            DS,
            DS((2, S)),
            DS,
            DS,
            DS,
            DS,
            DS,
        ],
        compiler_params=pltpu.CompilerParams(collective_id=0, has_side_effects=True),
    )(
        mrows,
        mgain.reshape(1, D),
        win.T,
        wgi.T,
        wgo.T,
        taps,
        wmo,
        rrows,
        rgain.reshape(1, D),
        ids.T,
        rw.T,
        eg,
        eu,
        ed,
    )
    return pl.pallas_call(
        put,
        out_shape=(
            jax.ShapeDtypeStruct((M, D), BF),
            jax.ShapeDtypeStruct((T, D), BF),
            pltpu.VMEM((M, D), BF),
            pltpu.VMEM((T, D), BF),
        ),
        in_specs=[VM, VM],
        out_specs=(HB, HB, VM, VM),
        scratch_shapes=[DS((2,))],
        input_output_aliases={0: 2, 1: 3},
    )(*results)[:2]


def solution(mesh):
    E = mesh.shape["ep"]
    Y = mesh.shape["tp"] // 2
    return jax.shard_map(
        functools.partial(on_device, E, Y),
        mesh=mesh,
        in_specs=(
            P("ep", None),
            P(),
            P(None, "tp"),
            P(None, "tp"),
            P(None, "tp"),
            P(None, "tp"),
            P("tp", None),
            P("ep", None),
            P(),
            P("ep", None),
            P("ep", None),
            P("ep", None, "tp"),
            P("ep", None, "tp"),
            P("ep", "tp", None),
        ),
        out_specs=(P("ep", None), P("ep", None)),
        check_vma=False,
    )
```
